32 devices in a mesh: kv: 8 (over z, y), tp: 4 (over x, core).
Axes of the slice: x: 2, y: 2, z: 4, core: 2. Of those that a mesh axis runs over, the one named last changes fastest.
Arguments:
- hidden_rows: bfloat16 [128, 4096], P('kv', 'tp'), may hold values from -16 to 16
- carried_state: float32 [128, 524288], P('kv', 'tp'), may hold values from -6 to 6
- norm_gain: bfloat16 [4096], replicated, may hold values from 0.099609375 to 1.8984375
- w_query: bfloat16 [4096, 2048], P('kv', 'tp'), may hold values from -0.09375 to 0.09375
- w_key: bfloat16 [4096, 2048], P('kv', 'tp'), may hold values from -0.09375 to 0.09375
- w_decay: bfloat16 [4096, 2048], P('kv', 'tp'), may hold values from -0.375 to 0.375
- w_value: bfloat16 [4096, 4096], P('kv', 'tp'), may hold values from -0.09375 to 0.09375
- w_gate: bfloat16 [4096, 4096], P('kv', 'tp'), may hold values from -0.09375 to 0.09375
- decay_bias: float32 [2048], P('tp'), may hold values from -32 to 8
- head_gain: bfloat16 [256], replicated, may hold values from 0.099609375 to 1.8984375
- w_out: bfloat16 [4096, 4096], P('tp', 'kv'), may hold values from -0.09375 to 0.09375
- mlp_gain: bfloat16 [4096], P('tp'), may hold values from 0.099609375 to 1.8984375
- w_up: bfloat16 [4096, 16384], P('tp', 'kv'), may hold values from -0.09375 to 0.09375
- w_down: bfloat16 [16384, 4096], P('kv', 'tp'), may hold values from -0.046875 to 0.046875
Outputs:
- updated_rows: bfloat16 [128, 4096], P('kv', 'tp')
- new_state: float32 [128, 524288], P('kv', 'tp')
The draws below stay inside these ranges and needn't reach their ends.
All inputs are finite; a program needn't handle non-finite values.
Results may differ from the reference program's by a relative error of at most 0.025.
Values may be sent and summed in bfloat16 or wider, within the bound.
A program may use at most 128 MiB of HBM per device.

```python
import jax
import jax.numpy as jnp
from jax import lax

D = 4096
HEADS = 16
DK = 128
DV = 256
FF = 16384
BATCH = 128
N_TP = 4


def draw_hidden_rows(key, part):
    key_base = jax.random.fold_in(key, 11)
    key_rough = jax.random.fold_in(key, 12)
    columns = jnp.arange(D, dtype=jnp.float32)
    rising = 0.5 * jnp.power(4.0, columns / D)
    rough = jnp.exp(jax.random.uniform(key_rough, (D,), jnp.float32, -0.35, 0.35))
    base = jnp.clip(jax.random.normal(key_base, (BATCH, D), jnp.float32), -5.0, 5.0)
    return (base * rising[None, :] * rough[None, :]).astype(jnp.bfloat16)


def shard_levels(rng, shape, pieces, smallest, largest):
    factor_of, own = 1.0, jax.random.fold_in(rng, 6)
    for dim, blocks in pieces:
        draws = jnp.exp(jax.random.uniform(jax.random.fold_in(own, dim), (blocks,), jnp.float32, smallest / len(pieces), largest / len(pieces)))
        factor_of = factor_of * jnp.repeat(draws, shape[dim] // blocks).reshape([-1 if axis == dim else 1 for axis in range(len(shape))])
    return factor_of


def normal_values(key, shape, deviation, bound, split=(), kind=jnp.bfloat16):
    entries = jax.random.normal(key, shape, jnp.float32) * deviation
    if len(split) > 0:
        entries = shard_levels(key, shape, split, -0.22, 0.18) * entries
    return jnp.clip(entries, min=-bound, max=bound).astype(kind)


def setup_inputs(seed: int = 0) -> dict:
    keys = jax.random.split(jax.random.key(seed), 15)
    hidden_rows = draw_hidden_rows(jax.random.fold_in(keys[14], 71), 0)
    carried_state = normal_values(keys[1], (BATCH, HEADS * DK * DV), 1.0, 6.0, ((0, 8), (1, 4)), jnp.float32)
    norm_gain = jnp.clip(1.0 + 0.18 * jax.random.normal(keys[2], (D,), jnp.float32), 0.099609375, 1.8984375).astype(jnp.bfloat16)
    w_query = normal_values(keys[3], (D, HEADS * DK), D ** -0.5, 0.09375, ((0, 8), (1, 4)))
    w_key = normal_values(keys[4], (D, HEADS * DK), D ** -0.5, 0.09375, ((0, 8), (1, 4)))
    w_decay = normal_values(keys[5], (D, HEADS * DK), (D // 16) ** -0.5, 0.375, ((0, 8), (1, 4)))
    w_value = normal_values(keys[6], (D, HEADS * DV), D ** -0.5, 0.09375, ((0, 8), (1, 4)))
    w_gate = normal_values(keys[7], (D, HEADS * DV), D ** -0.5, 0.09375, ((0, 8), (1, 4)))
    decay_bias = jnp.clip(-32.0 + 40.0 * jax.random.uniform(keys[8], (HEADS * DK,), jnp.float32) ** shard_levels(keys[8], (HEADS * DK,), ((0, 4),), -0.2, 0.2), -32.0, 8.0)
    head_gain = jnp.clip(1.0 + 0.18 * jax.random.normal(keys[9], (DV,), jnp.float32), 0.099609375, 1.8984375).astype(jnp.bfloat16)
    w_out = normal_values(keys[10], (HEADS * DV, D), (HEADS * DV) ** -0.5, 0.09375, ((0, 4), (1, 8)))
    mlp_gain = jnp.clip(1.0 + 0.18 * jax.random.normal(keys[11], (D,), jnp.float32), 0.099609375, 1.8984375).astype(jnp.bfloat16)
    w_up = normal_values(keys[12], (D, FF), D ** -0.5, 0.09375, ((0, 4), (1, 8)))
    w_down = normal_values(keys[13], (FF, D), FF ** -0.5, 0.046875, ((0, 8), (1, 4)))
    return dict(hidden_rows=hidden_rows, carried_state=carried_state, norm_gain=norm_gain, w_query=w_query, w_key=w_key, w_decay=w_decay, w_value=w_value, w_gate=w_gate, decay_bias=decay_bias, head_gain=head_gain, w_out=w_out, mlp_gain=mlp_gain, w_up=w_up, w_down=w_down)


epsilon = 1e-06
decay_normalizer = 16.0

def reference(hidden_rows, carried_state, norm_gain, w_query, w_key, w_decay, w_value, w_gate, decay_bias, head_gain, w_out, mlp_gain, w_up, w_down):
    batch_rows = hidden_rows.shape[0]
    inputs = hidden_rows.astype(jnp.float32)
    normed = (inputs * lax.rsqrt(lax.optimization_barrier(jnp.mean(inputs * inputs, axis=-1, keepdims=True)) + epsilon) * norm_gain.astype(jnp.float32)).astype(jnp.bfloat16)
    queries = jnp.dot(normed, w_query, preferred_element_type=jnp.float32).astype(jnp.bfloat16)
    keys_new = jnp.dot(normed, w_key, preferred_element_type=jnp.float32).astype(jnp.bfloat16)
    decay_pre = jnp.dot(normed, w_decay, preferred_element_type=jnp.float32).astype(jnp.bfloat16)
    values = jnp.dot(normed, w_value, preferred_element_type=jnp.float32).astype(jnp.bfloat16)
    out_gate = jnp.dot(normed, w_gate, preferred_element_type=jnp.float32).astype(jnp.bfloat16)
    log_decay = jax.nn.log_sigmoid(decay_pre.astype(jnp.float32) + decay_bias) / decay_normalizer
    log_decay = log_decay.reshape(batch_rows, HEADS, DK)
    carried = carried_state.reshape(batch_rows, HEADS, DK, DV)
    key_heads = keys_new.astype(jnp.float32).reshape(batch_rows, HEADS, DK)
    value_heads = values.astype(jnp.float32).reshape(batch_rows, HEADS, DV)
    new_state = jnp.exp(log_decay)[..., None] * carried + key_heads[..., None] * value_heads[..., None, :]
    query_heads = queries.astype(jnp.float32).reshape(batch_rows, HEADS, DK) * DK ** (-0.5)
    head_out = jnp.einsum('bhk,bhkv->bhv', query_heads, new_state, precision=lax.Precision.HIGHEST)
    gate_heads = out_gate.astype(jnp.float32).reshape(batch_rows, HEADS, DV)
    mixed = head_out * lax.rsqrt(lax.optimization_barrier(jnp.mean(head_out * head_out, axis=-1, keepdims=True)) + epsilon)
    mixed = (mixed * head_gain.astype(jnp.float32) * jax.nn.silu(gate_heads)).astype(jnp.bfloat16)
    mixed = mixed.reshape(batch_rows, HEADS * DV)
    group_rows = HEADS * DV // N_TP
    attn_total = jnp.zeros((batch_rows, D), jnp.float32)
    for block in range(N_TP):
        low = block * group_rows
        piece = jnp.dot(mixed[:, low:low + group_rows], w_out[low:low + group_rows], preferred_element_type=jnp.float32).astype(jnp.bfloat16)
        piece = lax.optimization_barrier(piece)
        attn_total = attn_total + piece.astype(jnp.float32)
    attn_out = attn_total.astype(jnp.bfloat16)
    residual = (inputs + attn_out.astype(jnp.float32)).astype(jnp.bfloat16)
    resid_float = residual.astype(jnp.float32)
    row_scale = lax.rsqrt(lax.optimization_barrier(jnp.mean(resid_float * resid_float, axis=-1, keepdims=True)) + epsilon)
    mlp_input = (resid_float * row_scale * mlp_gain.astype(jnp.float32)).astype(jnp.bfloat16)
    feature_block = D // N_TP
    up_sum = jnp.zeros((batch_rows, FF), jnp.float32)
    for block in range(N_TP):
        low = block * feature_block
        piece = jnp.dot(mlp_input[:, low:low + feature_block], w_up[low:low + feature_block], preferred_element_type=jnp.float32).astype(jnp.bfloat16)
        piece = lax.optimization_barrier(piece)
        up_sum = up_sum + piece.astype(jnp.float32)
    activation = jnp.square(jax.nn.relu(up_sum)).astype(jnp.bfloat16)
    mlp_out = jnp.dot(activation, w_down, preferred_element_type=jnp.float32).astype(jnp.bfloat16)
    updated_rows = (resid_float + mlp_out.astype(jnp.float32)).astype(jnp.bfloat16)
    return (updated_rows, new_state.reshape(batch_rows, HEADS * DK * DV))
```

```python
import functools

import jax
import jax.numpy as jnp
from jax import lax
from jax.experimental import pallas as pl
from jax.experimental.pallas import tpu as pltpu
from jax.sharding import PartitionSpec as P

DK = 128
DV = 256

epsilon = 1e-06
decay_normalizer = 16.0

F32 = jnp.float32
BF16 = jnp.bfloat16
MESH = pl.DeviceIdType.MESH
CHUNKS = 4
VMEM_BYTES = 67043328


def remote(src, dst, send_sem, recv_sem, i, j):
    return pltpu.make_async_remote_copy(
        src_ref=src,
        dst_ref=dst,
        send_sem=send_sem,
        recv_sem=recv_sem,
        device_id={"kv": i, "tp": j},
        device_id_type=MESH,
    )


def dot(a, b):
    return jnp.dot(a, b, preferred_element_type=F32)


def inner_size(kv):
    size = 1
    while (size * 2) ** 2 <= kv:
        size = size * 2
    return size


def layer_kernel(
    kv, tp,
    h_ref, ng_ref, bias_ref, hg_ref, mg_ref, wq, wk, wd_, wv, wg, old, wo, wu, wdn,
    out_ref, st_ref,
    vq, vk, vd_, vv, vg, vo, vu, vdn,
    xbuf, psnd, prcv, zsnd, zrcv, ssq, query, key, decay, value, head,
    mixed, mall, asend, arecv, rpart, rall, usend, urecv, xsend, xrecv, act, dsend, drecv, ssq2,
    wsem, stsem, hs_sem, hr_sem, ss_sem, sr_sem, ps_sem, pr_sem, qs_sem, qr_sem,
    ms_sem, mr_sem, as_sem, ar_sem, rs_sem, rr_sem, ts_sem, tr_sem,
    us_sem, ur_sem, xs_sem, xr_sem, cs_sem, cr_sem, ds_sem, dr_sem,
):
    i, j = lax.axis_index("kv"), lax.axis_index("tp")
    ny = inner_size(kv)
    nz = kv // ny
    z, y = i // ny, lax.rem(i, ny)
    ratio = kv // tp
    owner = i // ratio
    rows = h_ref.shape[0]
    columns = h_ref.shape[1]
    width = xbuf.shape[2]
    cw = vq.shape[1]
    heads = cw // DK
    sent = []

    def start(copy):
        copy.start()
        sent.append((copy, None))

    def start_if(condition, copy):
        pl.when(condition)(copy.start)
        sent.append((copy, condition))

    barrier = pltpu.get_barrier_semaphore()

    def greet(a, b):
        pl.semaphore_signal(
            barrier, inc=1, device_id={"kv": a, "tp": b}, device_id_type=MESH
        )

    for s in range(kv):
        k = lax.rem(i + s, kv)
        if s:
            greet(k, owner)
            greet(k, j)
        else:
            pl.when(owner != j)(lambda: greet(i, owner))
    for a in range(ratio):
        for s in range(tp):
            k, t = j * ratio + a, lax.rem(j + s, tp)
            if s:
                greet(k, t)
            else:
                pl.when(k != i)(functools.partial(greet, k, t))
    for s in range(1, tp):
        greet(i, lax.rem(j + s, tp))

    loads = [
        pltpu.make_async_copy(w, v, wsem.at[n])
        for n, (w, v) in enumerate(
            ((wd_, vd_), (wk, vk), (wq, vq), (wv, vv), (wg, vg), (wo, vo), (wu, vu), (wdn, vdn))
        )
    ]
    load_state = pltpu.make_async_copy(old, st_ref, stsem)
    for load in loads[:5]:
        load.start()
    load_state.start()
    for load in loads[5:]:
        load.start()

    hidden = h_ref[...].astype(F32)
    ssq[j] = jnp.broadcast_to(jnp.sum(hidden * hidden, axis=1, keepdims=True), (rows, 128))
    itself = jnp.where(owner == j, 1, 0)
    pl.semaphore_wait(barrier, 2 * (kv - itself) + (kv - 1) + (tp - 1))

    for a in range(ratio):
        for s in range(tp):
            k, t = j * ratio + a, lax.rem(j + s, tp)
            copy = remote(
                h_ref.at[:, pl.ds(a * width, width)], xbuf.at[i],
                hs_sem.at[a * tp + s], hr_sem.at[i], k, t,
            )
            if s:
                start(copy)
            else:
                start_if(k != i, copy)

                @pl.when(k == i)
                def _():
                    xbuf[i] = h_ref[:, a * width : (a + 1) * width]

    for s in range(1, tp):
        start(remote(ssq.at[j], ssq.at[j], ss_sem.at[s], sr_sem.at[j], i, lax.rem(j + s, tp)))

    gain = ng_ref[:, pl.ds(pl.multiple_of(i * width, 128), width)].astype(F32)
    for s in range(kv):
        k = lax.rem(i + s, kv)
        arrive = remote(xbuf.at[k], xbuf.at[k], hs_sem.at[0], hr_sem.at[k], k, owner)
        if s:
            arrive.wait_recv()
        else:
            pl.when(owner != j)(arrive.wait_recv)
    x = (xbuf[...].reshape(kv * rows, width).astype(F32) * gain).astype(BF16)

    pieces = []
    for n, v in enumerate((vd_, vk, vq, vv, vg)):
        for low in range(0, v.shape[1], cw):
            pieces.append((n, v, low))
    for c, (n, v, low) in enumerate(pieces):
        if low == 0:
            loads[n].wait()
        part = dot(x, v[:, low : low + cw]).astype(BF16)
        for zz in range(nz):
            for yy in range(ny):
                at = (zz * ny + yy) * rows
                psnd[c, yy, zz] = part[at : at + rows]
        for s in range(1, ny):
            yy = lax.rem(y + s, ny)
            start(
                remote(
                    psnd.at[c, yy], prcv.at[c, y], ps_sem.at[c, s], pr_sem.at[c, y], z * ny + yy, j
                )
            )

    def along_z(c):
        acc = psnd[c, y].astype(F32)
        for s in range(1, ny):
            yy = lax.rem(y + s, ny)
            at = prcv.at[c, yy]
            remote(at, at, ps_sem.at[c, 0], pr_sem.at[c, yy], z * ny + yy, j).wait_recv()
            acc = acc + prcv[c, yy].astype(F32)
        zsnd[c] = acc.astype(BF16)
        for s in range(1, nz):
            zz = lax.rem(z + s, nz)
            start(
                remote(
                    zsnd.at[c, zz], zrcv.at[c, z], qs_sem.at[c, s], qr_sem.at[c, z], zz * ny + y, j
                )
            )

    def reduced(c):
        acc = zsnd[c, z].astype(F32)
        for s in range(1, nz):
            zz = lax.rem(z + s, nz)
            at = zrcv.at[c, zz]
            remote(at, at, qs_sem.at[c, 0], qr_sem.at[c, zz], zz * ny + y, j).wait_recv()
            acc = acc + zrcv[c, zz].astype(F32)
        return (acc * scale).astype(BF16).astype(F32)

    for c in range(len(pieces)):
        along_z(c)
    for s in range(1, tp):
        k = lax.rem(j + s, tp)
        remote(ssq.at[k], ssq.at[k], ss_sem.at[0], sr_sem.at[k], i, k).wait_recv()
    total = ssq[0]
    for s in range(1, tp):
        total = total + ssq[s]
    scale = lax.rsqrt(total[:, :1] / (kv * width) + epsilon)

    pre = reduced(0) + bias_ref[...]
    log_decay = jnp.minimum(pre, 0.0) - jnp.log1p(jnp.exp(-jnp.abs(pre)))
    decay[...] = jnp.exp(log_decay / decay_normalizer)
    key[...] = reduced(1)
    query[...] = reduced(2) * DK ** (-0.5)
    for c in range(3, 5):
        value[:, (c - 3) * cw : (c - 2) * cw] = reduced(c)
    load_state.wait()

    @pl.loop(0, heads)
    def _(h):
        narrow = pl.ds(pl.multiple_of(h * DK, DK), DK)
        wide = pl.ds(pl.multiple_of(h * DV, DV), DV)
        q, k, d = query[:, narrow], key[:, narrow], decay[:, narrow]
        v = value[:, wide]
        acc = jnp.zeros((rows, DV), F32)
        for c in range(DK):
            at = pl.ds(pl.multiple_of(h * (DK * DV) + c * DV, DV), DV)
            new = d[:, c : c + 1] * st_ref[:, at] + k[:, c : c + 1] * v
            st_ref[:, at] = new
            acc = acc + q[:, c : c + 1] * new
        acc = acc * lax.rsqrt(jnp.mean(acc * acc, axis=1, keepdims=True) + epsilon)
        head[:, wide] = acc * hg_ref[...].astype(F32)

    for c in range(5, 7):
        at = slice((c - 5) * cw, (c - 4) * cw)
        mixed[:, at] = (head[:, at] * jax.nn.silu(reduced(c))).astype(BF16)

    def everyone(src_of, dst, send_sem, recv_sem):
        for s in range(1, kv):
            k = lax.rem(i + s, kv)
            start(remote(src_of(k), dst.at[i], send_sem.at[s], recv_sem.at[i], k, j))

    def arrived(dst, send_sem, recv_sem, s):
        k = lax.rem(i + s, kv)
        remote(dst.at[k], dst.at[k], send_sem.at[0], recv_sem.at[k], k, j).wait_recv()
        return k

    everyone(lambda k: mixed, mall, ms_sem, mr_sem)
    mall[i] = mixed[...]
    loads[5].wait()
    for s in range(1, kv):
        arrived(mall, ms_sem, mr_sem, s)
    part = dot(mall[...].reshape(kv * rows, mall.shape[2]), vo[...]).astype(BF16)
    asend[...] = part.reshape(asend.shape)
    for s in range(1, tp):
        t = lax.rem(j + s, tp)
        start(remote(asend.at[t], arecv.at[j], as_sem.at[s], ar_sem.at[j], i, t))
    attn = asend[j].astype(F32)
    for s in range(1, tp):
        t = lax.rem(j + s, tp)
        remote(arecv.at[t], arecv.at[t], as_sem.at[0], ar_sem.at[t], i, t).wait_recv()
        attn = attn + arecv[t].astype(F32)
    mine = xbuf[pl.ds(j * ratio, ratio)].reshape(ratio * rows, width).astype(F32)
    rpart[...] = (mine + attn.astype(BF16).astype(F32)).astype(BF16)

    slot = lax.rem(i, ratio)
    for s in range(kv):
        k = lax.rem(i + s, kv)
        copy = remote(rpart, rall.at[slot, j], rs_sem.at[s], rr_sem.at[slot, j], k, owner)
        if s:
            start(copy)
        else:
            start_if(owner != j, copy)

    @pl.when(owner == j)
    def _():
        rall[slot, j] = rpart[...]

    loads[6].wait()
    for a in range(ratio):
        k = j * ratio + a
        for s in range(tp):
            t = lax.rem(j + s, tp)
            at = rall.at[a, t]
            arrive = remote(at, at, rs_sem.at[0], rr_sem.at[a, t], k, t)
            if s:
                arrive.wait_recv()
            else:
                pl.when(k != i)(arrive.wait_recv)

    def own(a):
        return rall[a, owner, pl.ds(pl.multiple_of(slot * rows, rows), rows), :]

    squares = None
    for a in range(ratio):
        term = own(a).astype(F32)
        term = jnp.sum(term * term, axis=1, keepdims=True)
        squares = term if squares is None else squares + term
    ssq2[j] = jnp.broadcast_to(squares, (rows, 128))
    for s in range(1, tp):
        start(remote(ssq2.at[j], ssq2.at[j], ts_sem.at[s], tr_sem.at[j], i, lax.rem(j + s, tp)))
    x = jnp.concatenate(
        [
            (
                rall[a].reshape(kv * rows, width).astype(F32)
                * mg_ref[:, a * width : (a + 1) * width].astype(F32)
            ).astype(BF16)
            for a in range(ratio)
        ],
        axis=1,
    )

    half = vu.shape[1] // 2
    chunks = usend.shape[0]
    piece = half // chunks
    core, across = lax.rem(j, 2), j // 2
    other = 1 - core
    partner = across * 2 + other

    def columns_of(h, c):
        return pl.ds(pl.multiple_of(h * half + c * piece, 128), piece)

    def give(c):
        usend[c] = dot(x, vu[:, columns_of(other, c)]).astype(BF16)
        start(remote(usend.at[c], urecv.at[c], us_sem.at[c], ur_sem.at[c], i, partner))

    give(0)
    for c in range(chunks):
        if c + 1 < chunks:
            give(c + 1)
        mine = dot(x, vu[:, columns_of(core, c)])
        remote(urecv.at[c], urecv.at[c], us_sem.at[c], ur_sem.at[c], i, partner).wait_recv()
        xsend[c] = (mine + urecv[c].astype(F32)).astype(BF16)
        for s in range(1, tp // 2):
            to = lax.rem(across + s, tp // 2)
            start(
                remote(
                    xsend.at[c], xrecv.at[across, c], xs_sem.at[s, c], xr_sem.at[across, c],
                    i, to * 2 + core,
                )
            )
    loads[7].wait()
    down = None
    for c in range(chunks):
        total = xsend[c].astype(F32)
        for s in range(1, tp // 2):
            at = lax.rem(across + s, tp // 2)
            slot_ref = xrecv.at[at, c]
            remote(
                slot_ref, slot_ref, xs_sem.at[0, c], xr_sem.at[at, c], i, at * 2 + core
            ).wait_recv()
            total = total + xrecv[at, c].astype(F32)
        act[core, c] = jnp.square(jnp.maximum(total, 0.0)).astype(BF16)
        start(
            remote(act.at[core, c], act.at[core, c], cs_sem.at[c], cr_sem.at[core, c], i, partner)
        )
        term = dot(act[core, c], vdn[columns_of(core, c), :])
        down = term if down is None else down + term
        arrive = act.at[other, c]
        remote(arrive, arrive, cs_sem.at[c], cr_sem.at[other, c], i, partner).wait_recv()
        down = down + dot(act[other, c], vdn[columns_of(other, c), :])
    dsend[...] = down.astype(BF16).reshape(dsend.shape)
    everyone(lambda k: dsend.at[k], drecv, ds_sem, dr_sem)

    for s in range(1, tp):
        k = lax.rem(j + s, tp)
        remote(ssq2.at[k], ssq2.at[k], ts_sem.at[0], tr_sem.at[k], i, k).wait_recv()
    squares = ssq2[0]
    for s in range(1, tp):
        squares = squares + ssq2[s]
    scale2 = lax.rsqrt(squares[:, :1] / (columns * tp) + epsilon)
    acc = dsend[i].astype(F32)
    for s in range(1, kv):
        k = arrived(drecv, ds_sem, dr_sem, s)
        acc = acc + drecv[k].astype(F32)
    acc = (acc * (scale2 * scale2)).astype(BF16).astype(F32)
    for a in range(ratio):
        at = slice(a * width, (a + 1) * width)
        out_ref[:, at] = (own(a).astype(F32) + acc[:, at]).astype(BF16)
    for copy, condition in sent:
        if condition is None:
            copy.wait_send()
        else:
            pl.when(condition)(copy.wait_send)


def layer(
    kv, tp, hidden_rows, carried, norm_gain, weights, decay_bias, head_gain, w_out, mlp_gain,
    w_up, w_down,
):
    rows, columns = hidden_rows.shape
    width = w_out.shape[1]
    ratio = kv // tp
    ny = inner_size(kv)
    nz = kv // ny
    cw = weights[0].shape[1]
    wide = weights[3].shape[1]
    pieces = sum(w.shape[1] for w in weights) // cw
    half = w_up.shape[1] // 2
    everything = kv * rows
    chunks = max(1, min(CHUNKS, half // 128))
    limit = VMEM_BYTES - 4 * carried.size - 128 * 1024
    vmem = pl.BlockSpec(memory_space=pltpu.VMEM)
    hbm = pl.BlockSpec(memory_space=pltpu.HBM)
    dma = pltpu.SemaphoreType.DMA
    wq, wk, wd_, wv, wg = weights
    return pl.pallas_call(
        functools.partial(layer_kernel, kv, tp),
        out_shape=[
            jax.ShapeDtypeStruct((rows, columns), BF16),
            pltpu.VMEM(carried.shape, F32),
        ],
        in_specs=[vmem] * 5 + [hbm] * 9,
        out_specs=[vmem, vmem],
        scratch_shapes=[
            pltpu.VMEM(w.shape, BF16) for w in (wq, wk, wd_, wv, wg, w_out, w_up, w_down)
        ]
        + [
            pltpu.VMEM((kv, rows, width), BF16),
            pltpu.VMEM((pieces, ny, nz, rows, cw), BF16),
            pltpu.VMEM((pieces, ny, nz, rows, cw), BF16),
            pltpu.VMEM((pieces, nz, rows, cw), BF16),
            pltpu.VMEM((pieces, nz, rows, cw), BF16),
            pltpu.VMEM((tp, rows, 128), F32),
            pltpu.VMEM((rows, cw), F32),
            pltpu.VMEM((rows, cw), F32),
            pltpu.VMEM((rows, cw), F32),
            pltpu.VMEM((rows, wide), F32),
            pltpu.VMEM((rows, wide), F32),
            pltpu.VMEM((rows, wide), BF16),
            pltpu.VMEM((kv, rows, wide), BF16),
            pltpu.VMEM((tp, ratio * rows, width), BF16),
            pltpu.VMEM((tp, ratio * rows, width), BF16),
            pltpu.VMEM((ratio * rows, width), BF16),
            pltpu.VMEM((ratio, tp, ratio * rows, width), BF16),
            pltpu.VMEM((chunks, everything, half // chunks), BF16),
            pltpu.VMEM((chunks, everything, half // chunks), BF16),
            pltpu.VMEM((chunks, everything, half // chunks), BF16),
            pltpu.VMEM((tp // 2, chunks, everything, half // chunks), BF16),
            pltpu.VMEM((2, chunks, everything, half // chunks), BF16),
            pltpu.VMEM((kv, rows, columns), BF16),
            pltpu.VMEM((kv, rows, columns), BF16),
            pltpu.VMEM((tp, rows, 128), F32),
            dma((8,)),
            dma,
            dma((kv,)),
            dma((kv,)),
            dma((tp,)),
            dma((tp,)),
            dma((pieces, ny)),
            dma((pieces, ny)),
            dma((pieces, nz)),
            dma((pieces, nz)),
            dma((kv,)),
            dma((kv,)),
            dma((tp,)),
            dma((tp,)),
            dma((kv,)),
            dma((ratio, tp)),
            dma((tp,)),
            dma((tp,)),
            dma((chunks,)),
            dma((chunks,)),
            dma((tp // 2, chunks)),
            dma((tp // 2, chunks)),
            dma((chunks,)),
            dma((2, chunks)),
            dma((kv,)),
            dma((kv,)),
        ],
        compiler_params=pltpu.CompilerParams(
            has_side_effects=True, collective_id=0, vmem_limit_bytes=limit
        ),
        name="layer",
    )(
        hidden_rows, norm_gain.reshape(1, -1), decay_bias.reshape(1, -1),
        head_gain.reshape(1, -1), mlp_gain.reshape(1, -1), wq, wk, wd_, wv, wg, carried,
        w_out, w_up, w_down,
    )


def body(
    kv,
    tp,
    hidden_rows,
    carried_state,
    norm_gain,
    w_query,
    w_key,
    w_decay,
    w_value,
    w_gate,
    decay_bias,
    head_gain,
    w_out,
    mlp_gain,
    w_up,
    w_down,
):
    updated_rows, new_state = layer(
        kv, tp, hidden_rows, carried_state, norm_gain,
        (w_query, w_key, w_decay, w_value, w_gate), decay_bias, head_gain, w_out, mlp_gain,
        w_up, w_down,
    )
    return (updated_rows, new_state)


def solution(mesh):
    return jax.shard_map(
        functools.partial(body, mesh.shape["kv"], mesh.shape["tp"]),
        mesh=mesh,
        in_specs=(
            P("kv", "tp"),
            P("kv", "tp"),
            P(),
            P("kv", "tp"),
            P("kv", "tp"),
            P("kv", "tp"),
            P("kv", "tp"),
            P("kv", "tp"),
            P("tp"),
            P(),
            P("tp", "kv"),
            P("tp"),
            P("tp", "kv"),
            P("kv", "tp"),
        ),
        out_specs=(P("kv", "tp"), P("kv", "tp")),
        check_vma=False,
    )
```

```python
import functools

import jax
import jax.numpy as jnp
from jax import lax
from jax.experimental import pallas as pl
from jax.experimental.pallas import tpu as pltpu
from jax.sharding import PartitionSpec as P

DK = 128
DV = 256

epsilon = 1e-06
decay_normalizer = 16.0

F32 = jnp.float32
BF16 = jnp.bfloat16
MESH = pl.DeviceIdType.MESH
CHUNKS = 2
STORES = 8
VMEM_BYTES = 67043328


def remote(src, dst, send_sem, recv_sem, i, j):
    return pltpu.make_async_remote_copy(
        src_ref=src,
        dst_ref=dst,
        send_sem=send_sem,
        recv_sem=recv_sem,
        device_id={"kv": i, "tp": j},
        device_id_type=MESH,
    )


def dot(a, b):
    return jnp.dot(a, b, preferred_element_type=F32)


def inner_size(kv):
    size = 1
    while (size * 2) ** 2 <= kv:
        size = size * 2
    return size


def layer_kernel(
    kv, tp,
    h_in, ng_in, bias_in, hg_in, mg_in, wq, wk, wd_, wv, wg, old, wo, wu, wdn,
    out_ref, st_ref,
    h_ref, ng_ref, bias_ref, hg_ref, mg_ref, gains,
    vq, vk, vd_, vv, vg, vo, vu, vdn,
    xbuf, psnd, prcv, zsnd, zrcv, ssq, query, key, decay, value, head,
    mixed, mall, asend, arecv, rpart, rall, usend, urecv, xsend, xrecv, act, dsend, drecv, ssq2,
    insem, wsem, stsem, hs_sem, hr_sem, fs_sem, ss_sem, sr_sem, ps_sem, pr_sem, qs_sem, qr_sem,
    ms_sem, mr_sem, as_sem, ar_sem, rs_sem, rr_sem, ts_sem, tr_sem,
    us_sem, ur_sem, xs_sem, xr_sem, cs_sem, cr_sem, ds_sem, dr_sem,
):
    i, j = lax.axis_index("kv"), lax.axis_index("tp")
    ny = inner_size(kv)
    nz = kv // ny
    z, y = i // ny, lax.rem(i, ny)
    ratio = kv // tp
    owner = i // ratio
    rows = h_ref.shape[0]
    columns = h_ref.shape[1]
    width = xbuf.shape[2]
    cw = vq.shape[1]
    heads = cw // DK
    sent = []

    def start(copy):
        copy.start()
        sent.append((copy, None))

    def start_if(condition, copy):
        pl.when(condition)(copy.start)
        sent.append((copy, condition))

    inputs = [
        pltpu.make_async_copy(src, dst, insem.at[n])
        for n, (src, dst) in enumerate(
            ((h_in, h_ref), (ng_in, ng_ref), (bias_in, bias_ref), (hg_in, hg_ref), (mg_in, mg_ref))
        )
    ]
    for copy in inputs:
        copy.start()
    barrier = pltpu.get_barrier_semaphore()

    def greet(a, b):
        pl.semaphore_signal(
            barrier, inc=1, device_id={"kv": a, "tp": b}, device_id_type=MESH
        )

    for s in range(kv):
        k = lax.rem(i + s, kv)
        if s:
            greet(k, owner)
            greet(k, j)
        else:
            pl.when(owner != j)(lambda: greet(i, owner))
    for a in range(ratio):
        for s in range(tp):
            k, t = j * ratio + a, lax.rem(j + s, tp)
            if s:
                greet(k, t)
            else:
                pl.when(k != i)(functools.partial(greet, k, t))
    for s in range(1, tp):
        greet(i, lax.rem(j + s, tp))

    loads = [
        pltpu.make_async_copy(w, v, wsem.at[n])
        for n, (w, v) in enumerate(
            ((wd_, vd_), (wk, vk), (wq, vq), (wv, vv), (wg, vg), (wo, vo), (wu, vu), (wdn, vdn))
        )
    ]
    load_state = pltpu.make_async_copy(old, st_ref, stsem)
    for load in loads[:5]:
        load.start()
    load_state.start()
    for load in loads[5:]:
        load.start()

    for copy in inputs:
        copy.wait()
    hidden = h_ref[...].astype(F32)
    ssq[j] = jnp.broadcast_to(jnp.sum(hidden * hidden, axis=1, keepdims=True), (rows, 128))
    itself = jnp.where(owner == j, 1, 0)
    pl.semaphore_wait(barrier, 2 * (kv - itself) + (kv - 1) + (tp - 1))

    side = lax.rem(i, 2)
    for a in range(ratio):
        k = j * ratio + a
        src = h_ref.at[:, pl.ds(a * width, width)]
        for s in range(tp // 2):
            t = lax.rem(j // 2 + s, tp // 2) * 2 + side
            copy = remote(src, xbuf.at[i], hs_sem.at[a * (tp // 2) + s], hr_sem.at[i], k, t)
            if s:
                start(copy)
            else:
                start_if(jnp.logical_or(k != i, t != j), copy)

                @pl.when(jnp.logical_and(k == i, t == j))
                def _():
                    xbuf[i] = h_ref[:, a * width : (a + 1) * width]

    for s in range(1, tp):
        start(remote(ssq.at[j], ssq.at[j], ss_sem.at[s], sr_sem.at[j], i, lax.rem(j + s, tp)))

    gains[...] = ng_ref[...].astype(F32).reshape(1, kv * width)
    gain = gains[:, pl.ds(pl.multiple_of(i * width, 128), width)]
    core = lax.rem(j, 2)
    partner = j + 1 - 2 * core
    even = i - lax.rem(i, 2)
    for s in range(kv // 2):
        k = lax.rem(even + 2 * s, kv) + core
        arrive = remote(xbuf.at[k], xbuf.at[k], hs_sem.at[0], hr_sem.at[k], k, owner)
        if s:
            arrive.wait_recv()
        else:
            pl.when(jnp.logical_or(owner != j, k != i))(arrive.wait_recv)
        start(remote(xbuf.at[k], xbuf.at[k], fs_sem.at[s], hr_sem.at[k], i, partner))
    for s in range(kv // 2):
        k = lax.rem(even + 2 * s, kv) + 1 - core
        remote(xbuf.at[k], xbuf.at[k], fs_sem.at[0], hr_sem.at[k], i, partner).wait_recv()
    x = (xbuf[...].reshape(kv * rows, width).astype(F32) * gain).astype(BF16)

    pieces = []
    for n, v in enumerate((vd_, vk, vq, vv, vg)):
        for low in range(0, v.shape[1], cw):
            pieces.append((n, v, low))
    for c, (n, v, low) in enumerate(pieces):
        if low == 0:
            loads[n].wait()
        part = dot(x, v[:, low : low + cw]).astype(BF16)
        for zz in range(nz):
            for yy in range(ny):
                at = (zz * ny + yy) * rows
                psnd[c, yy, zz] = part[at : at + rows]
        for s in range(1, ny):
            yy = lax.rem(y + s, ny)
            start(
                remote(
                    psnd.at[c, yy], prcv.at[c, y], ps_sem.at[c, s], pr_sem.at[c, y], z * ny + yy, j
                )
            )

    def along_z(c):
        acc = psnd[c, y].astype(F32)
        for s in range(1, ny):
            yy = lax.rem(y + s, ny)
            at = prcv.at[c, yy]
            remote(at, at, ps_sem.at[c, 0], pr_sem.at[c, yy], z * ny + yy, j).wait_recv()
            acc = acc + prcv[c, yy].astype(F32)
        zsnd[c] = acc.astype(BF16)
        for s in range(1, nz):
            zz = lax.rem(z + s, nz)
            start(
                remote(
                    zsnd.at[c, zz], zrcv.at[c, z], qs_sem.at[c, s], qr_sem.at[c, z], zz * ny + y, j
                )
            )

    def reduced(c):
        acc = zsnd[c, z].astype(F32)
        for s in range(1, nz):
            zz = lax.rem(z + s, nz)
            at = zrcv.at[c, zz]
            remote(at, at, qs_sem.at[c, 0], qr_sem.at[c, zz], zz * ny + y, j).wait_recv()
            acc = acc + zrcv[c, zz].astype(F32)
        return (acc * scale).astype(BF16).astype(F32)

    for c in range(len(pieces)):
        along_z(c)
    for s in range(1, tp):
        k = lax.rem(j + s, tp)
        remote(ssq.at[k], ssq.at[k], ss_sem.at[0], sr_sem.at[k], i, k).wait_recv()
    total = ssq[0]
    for s in range(1, tp):
        total = total + ssq[s]
    scale = lax.rsqrt(total[:, :1] / (kv * width) + epsilon)

    pre = reduced(0) + bias_ref[...]
    log_decay = jnp.minimum(pre, 0.0) - jnp.log1p(jnp.exp(-jnp.abs(pre)))
    decay[...] = jnp.exp(log_decay / decay_normalizer)
    key[...] = reduced(1)
    query[...] = reduced(2) * DK ** (-0.5)
    load_state.wait()

    def head_slices(h):
        narrow = pl.ds(pl.multiple_of(h * DK, DK), DK)
        wide = pl.ds(pl.multiple_of(h * DV, DV), DV)
        return narrow, wide

    def state_slice(h, c):
        return pl.ds(pl.multiple_of(h * (DK * DV) + c * DV, DV), DV)

    @pl.loop(0, heads)
    def _(h):
        narrow, wide = head_slices(h)
        q = query[:, narrow] * decay[:, narrow]
        acc = jnp.zeros((rows, DV), F32)
        for c in range(DK):
            acc = acc + q[:, c : c + 1] * st_ref[:, state_slice(h, c)]
        head[:, wide] = acc

    for c in range(3, 5):
        value[:, (c - 3) * cw : (c - 2) * cw] = reduced(c)
    head_gain = hg_ref[...].astype(F32).reshape(1, DV)
    for h in range(heads):
        at = slice(h * DK, (h + 1) * DK)
        weight = jnp.sum(query[:, at] * key[:, at], axis=1, keepdims=True)
        at = slice(h * DV, (h + 1) * DV)
        acc = head[:, at] + weight * value[:, at]
        acc = acc * lax.rsqrt(jnp.mean(acc * acc, axis=1, keepdims=True) + epsilon)
        head[:, at] = acc * head_gain

    for c in range(5, 7):
        at = slice((c - 5) * cw, (c - 4) * cw)
        mixed[:, at] = (head[:, at] * jax.nn.silu(reduced(c))).astype(BF16)

    def everyone(src_of, dst, send_sem, recv_sem):
        for s in range(1, kv):
            k = lax.rem(i + s, kv)
            start(remote(src_of(k), dst.at[i], send_sem.at[s], recv_sem.at[i], k, j))

    def arrived(dst, send_sem, recv_sem, s):
        k = lax.rem(i + s, kv)
        remote(dst.at[k], dst.at[k], send_sem.at[0], recv_sem.at[k], k, j).wait_recv()
        return k

    everyone(lambda k: mixed, mall, ms_sem, mr_sem)
    mall[i] = mixed[...]

    loads[5].wait()
    for s in range(1, kv):
        arrived(mall, ms_sem, mr_sem, s)
    part = dot(mall[...].reshape(kv * rows, mall.shape[2]), vo[...]).astype(BF16)
    asend[...] = part.reshape(asend.shape)
    for s in range(1, tp):
        t = lax.rem(j + s, tp)
        start(remote(asend.at[t], arecv.at[j], as_sem.at[s], ar_sem.at[j], i, t))
    attn = asend[j].astype(F32)
    for s in range(1, tp):
        t = lax.rem(j + s, tp)
        remote(arecv.at[t], arecv.at[t], as_sem.at[0], ar_sem.at[t], i, t).wait_recv()
        attn = attn + arecv[t].astype(F32)
    mine = xbuf[pl.ds(j * ratio, ratio)].reshape(ratio * rows, width).astype(F32)
    res = (mine + attn.astype(BF16).astype(F32)).astype(BF16)
    for m in range(ratio):
        rpart[m % 2, m // 2 * rows : (m // 2 + 1) * rows] = res[m * rows : (m + 1) * rows]

    slot = lax.rem(i, ratio)
    for p in range(2):
        for s in range(kv):
            k = lax.rem(i + s, kv)
            copy = remote(
                rpart.at[p], rall.at[slot, p, j], rs_sem.at[p, s], rr_sem.at[slot, p, j], k, owner
            )
            if s:
                start(copy)
            else:
                start_if(owner != j, copy)

    @pl.when(owner == j)
    def _():
        for p in range(2):
            rall[slot, p, j] = rpart[p]

    @pl.loop(0, heads)
    def _(h):
        narrow, wide = head_slices(h)
        k, d = key[:, narrow], decay[:, narrow]
        v = value[:, wide]
        for c in range(DK):
            at = state_slice(h, c)
            st_ref[:, at] = d[:, c : c + 1] * st_ref[:, at] + k[:, c : c + 1] * v

    loads[6].wait()
    mlp_gain = mg_ref[...].astype(F32).reshape(1, columns)
    tokens = kv // 2 * rows

    def gathered(p):
        for a in range(ratio):
            k = j * ratio + a
            for s in range(tp):
                t = lax.rem(j + s, tp)
                at = rall.at[a, p, t]
                arrive = remote(at, at, rs_sem.at[p, 0], rr_sem.at[a, p, t], k, t)
                if s:
                    arrive.wait_recv()
                else:
                    pl.when(k != i)(arrive.wait_recv)
        return jnp.concatenate(
            [
                (
                    rall[a, p].reshape(tokens, width).astype(F32)
                    * mlp_gain[:, a * width : (a + 1) * width]
                ).astype(BF16)
                for a in range(ratio)
            ],
            axis=1,
        )

    def own(a):
        low = pl.multiple_of(slot // 2 * rows, rows)
        return rall[a, lax.rem(slot, 2), owner, pl.ds(low, rows), :]

    half = vu.shape[1] // 2
    chunks = usend.shape[1]
    piece = half // chunks
    across = j // 2
    other = 1 - core

    def columns_of(h, c):
        return pl.ds(pl.multiple_of(h * half + c * piece, 128), piece)

    def up(p, x):
        def give(c):
            usend[p, c] = dot(x, vu[:, columns_of(other, c)]).astype(BF16)
            start(
                remote(
                    usend.at[p, c], urecv.at[p, c], us_sem.at[p, c], ur_sem.at[p, c], i, partner
                )
            )

        give(0)
        for c in range(chunks):
            if c + 1 < chunks:
                give(c + 1)
            mine = dot(x, vu[:, columns_of(core, c)])
            at = urecv.at[p, c]
            remote(at, at, us_sem.at[p, c], ur_sem.at[p, c], i, partner).wait_recv()
            xsend[p, c] = (mine + urecv[p, c].astype(F32)).astype(BF16)
            for s in range(1, tp // 2):
                to = lax.rem(across + s, tp // 2)
                start(
                    remote(
                        xsend.at[p, c], xrecv.at[p, across, c],
                        xs_sem.at[p, s, c], xr_sem.at[p, across, c], i, to * 2 + core,
                    )
                )

    def down(p):
        acc = None
        for c in range(chunks):
            total = xsend[p, c].astype(F32)
            for s in range(1, tp // 2):
                at = lax.rem(across + s, tp // 2)
                ref = xrecv.at[p, at, c]
                remote(
                    ref, ref, xs_sem.at[p, 0, c], xr_sem.at[p, at, c], i, at * 2 + core
                ).wait_recv()
                total = total + xrecv[p, at, c].astype(F32)
            act[p, core, c] = jnp.square(jnp.maximum(total, 0.0)).astype(BF16)
            ref = act.at[p, core, c]
            start(remote(ref, ref, cs_sem.at[p, c], cr_sem.at[p, core, c], i, partner))
            term = dot(act[p, core, c], vdn[columns_of(core, c), :])
            acc = term if acc is None else acc + term
            ref = act.at[p, other, c]
            remote(ref, ref, cs_sem.at[p, c], cr_sem.at[p, other, c], i, partner).wait_recv()
            acc = acc + dot(act[p, other, c], vdn[columns_of(other, c), :])
        dsend[p] = acc.astype(BF16).reshape(dsend.shape[1:])
        for s in range(kv // 2):
            kk = lax.rem(i // 2 + s, kv // 2)
            k = 2 * kk + p
            copy = remote(dsend.at[p, kk], drecv.at[i], ds_sem.at[p, s], dr_sem.at[i], k, j)
            if s:
                start(copy)
            else:
                start_if(k != i, copy)

    up(0, gathered(0))
    x1 = gathered(1)
    squares = None
    for a in range(ratio):
        term = own(a).astype(F32)
        term = jnp.sum(term * term, axis=1, keepdims=True)
        squares = term if squares is None else squares + term
    ssq2[j] = jnp.broadcast_to(squares, (rows, 128))
    for s in range(1, tp):
        start(remote(ssq2.at[j], ssq2.at[j], ts_sem.at[s], tr_sem.at[j], i, lax.rem(j + s, tp)))
    up(1, x1)
    loads[7].wait()
    down(0)
    down(1)

    for s in range(1, tp):
        k = lax.rem(j + s, tp)
        remote(ssq2.at[k], ssq2.at[k], ts_sem.at[0], tr_sem.at[k], i, k).wait_recv()
    squares = ssq2[0]
    for s in range(1, tp):
        squares = squares + ssq2[s]
    scale2 = lax.rsqrt(squares[:, :1] / (columns * tp) + epsilon)
    acc = dsend[lax.rem(i, 2), i // 2].astype(F32)
    for s in range(1, kv):
        k = arrived(drecv, ds_sem.at[0], dr_sem, s)
        acc = acc + drecv[k].astype(F32)
    acc = (acc * (scale2 * scale2)).astype(BF16).astype(F32)
    for a in range(ratio):
        at = slice(a * width, (a + 1) * width)
        out_ref[:, at] = (own(a).astype(F32) + acc[:, at]).astype(BF16)
    for copy, condition in sent:
        if condition is None:
            copy.wait_send()
        else:
            pl.when(condition)(copy.wait_send)


def layer(
    kv, tp, hidden_rows, carried, norm_gain, weights, decay_bias, head_gain, w_out, mlp_gain,
    w_up, w_down,
):
    rows, columns = hidden_rows.shape
    width = w_out.shape[1]
    ratio = kv // tp
    ny = inner_size(kv)
    nz = kv // ny
    cw = weights[0].shape[1]
    wide = weights[3].shape[1]
    pieces = sum(w.shape[1] for w in weights) // cw
    half = w_up.shape[1] // 2
    tokens = kv // 2 * rows
    chunks = max(1, min(CHUNKS, half // 128))
    piece = half // chunks
    limit = VMEM_BYTES - 4 * carried.size - 128 * 1024
    vmem = pl.BlockSpec(memory_space=pltpu.VMEM)
    hbm = pl.BlockSpec(memory_space=pltpu.HBM)
    dma = pltpu.SemaphoreType.DMA
    wq, wk, wd_, wv, wg = weights
    bias = decay_bias.reshape(1, -1)
    return pl.pallas_call(
        functools.partial(layer_kernel, kv, tp),
        out_shape=[
            pltpu.VMEM((rows, columns), BF16),
            pltpu.VMEM(carried.shape, F32),
        ],
        in_specs=[hbm] * 14,
        out_specs=[vmem, vmem],
        scratch_shapes=[
            pltpu.VMEM(a.shape, a.dtype)
            for a in (hidden_rows, norm_gain, bias, head_gain, mlp_gain)
        ]
        + [pltpu.VMEM((1, norm_gain.shape[0]), F32)]
        + [
            pltpu.VMEM(w.shape, BF16) for w in (wq, wk, wd_, wv, wg, w_out, w_up, w_down)
        ]
        + [
            pltpu.VMEM((kv, rows, width), BF16),
            pltpu.VMEM((pieces, ny, nz, rows, cw), BF16),
            pltpu.VMEM((pieces, ny, nz, rows, cw), BF16),
            pltpu.VMEM((pieces, nz, rows, cw), BF16),
            pltpu.VMEM((pieces, nz, rows, cw), BF16),
            pltpu.VMEM((tp, rows, 128), F32),
            pltpu.VMEM((rows, cw), F32),
            pltpu.VMEM((rows, cw), F32),
            pltpu.VMEM((rows, cw), F32),
            pltpu.VMEM((rows, wide), F32),
            pltpu.VMEM((rows, wide), F32),
            pltpu.VMEM((rows, wide), BF16),
            pltpu.VMEM((kv, rows, wide), BF16),
            pltpu.VMEM((tp, ratio * rows, width), BF16),
            pltpu.VMEM((tp, ratio * rows, width), BF16),
            pltpu.VMEM((2, ratio // 2 * rows, width), BF16),
            pltpu.VMEM((ratio, 2, tp, ratio // 2 * rows, width), BF16),
            pltpu.VMEM((2, chunks, tokens, piece), BF16),
            pltpu.VMEM((2, chunks, tokens, piece), BF16),
            pltpu.VMEM((2, chunks, tokens, piece), BF16),
            pltpu.VMEM((2, tp // 2, chunks, tokens, piece), BF16),
            pltpu.VMEM((2, 2, chunks, tokens, piece), BF16),
            pltpu.VMEM((2, kv // 2, rows, columns), BF16),
            pltpu.VMEM((kv, rows, columns), BF16),
            pltpu.VMEM((tp, rows, 128), F32),
            dma((5,)),
            dma((8,)),
            dma,
            dma((kv,)),
            dma((kv,)),
            dma((kv,)),
            dma((tp,)),
            dma((tp,)),
            dma((pieces, ny)),
            dma((pieces, ny)),
            dma((pieces, nz)),
            dma((pieces, nz)),
            dma((kv,)),
            dma((kv,)),
            dma((tp,)),
            dma((tp,)),
            dma((2, kv)),
            dma((ratio, 2, tp)),
            dma((tp,)),
            dma((tp,)),
            dma((2, chunks)),
            dma((2, chunks)),
            dma((2, tp // 2, chunks)),
            dma((2, tp // 2, chunks)),
            dma((2, chunks)),
            dma((2, 2, chunks)),
            dma((2, kv // 2)),
            dma((kv,)),
        ],
        compiler_params=pltpu.CompilerParams(
            has_side_effects=True, collective_id=0, vmem_limit_bytes=limit
        ),
        name="layer",
    )(
        hidden_rows, norm_gain, bias, head_gain, mlp_gain, wq, wk, wd_, wv, wg, carried,
        w_out, w_up, w_down,
    )


def store_kernel(parts, new_in, rows_in, new_out, rows_out, sems):
    size = new_in.shape[1] // parts
    copies = [pltpu.make_async_copy(rows_in, rows_out, sems.at[parts])]
    for n in range(parts):
        at = pl.ds(n * size, size)
        copies.append(pltpu.make_async_copy(new_in.at[:, at], new_out.at[:, at], sems.at[n]))
    for copy in copies:
        copy.start()
    for copy in copies:
        copy.wait()


def store(updated_rows, new_state):
    parts = STORES
    vmem = pl.BlockSpec(memory_space=pltpu.VMEM)
    hbm = pl.BlockSpec(memory_space=pltpu.HBM)
    return pl.pallas_call(
        functools.partial(store_kernel, parts),
        out_shape=[
            jax.ShapeDtypeStruct(new_state.shape, new_state.dtype),
            jax.ShapeDtypeStruct(updated_rows.shape, updated_rows.dtype),
        ],
        in_specs=[vmem, vmem],
        out_specs=[hbm, hbm],
        scratch_shapes=[pltpu.SemaphoreType.DMA((parts + 1,))],
        compiler_params=pltpu.CompilerParams(vmem_limit_bytes=1024 * 1024),
        name="store",
    )(new_state, updated_rows)


def body(
    kv,
    tp,
    hidden_rows,
    carried_state,
    norm_gain,
    w_query,
    w_key,
    w_decay,
    w_value,
    w_gate,
    decay_bias,
    head_gain,
    w_out,
    mlp_gain,
    w_up,
    w_down,
):
    updated_rows, new_state = layer(
        kv, tp, hidden_rows, carried_state, norm_gain,
        (w_query, w_key, w_decay, w_value, w_gate), decay_bias, head_gain, w_out, mlp_gain,
        w_up, w_down,
    )
    new_state, updated_rows = store(updated_rows, new_state)
    return (updated_rows, new_state)


def solution(mesh):
    return jax.shard_map(
        functools.partial(body, mesh.shape["kv"], mesh.shape["tp"]),
        mesh=mesh,
        in_specs=(
            P("kv", "tp"),
            P("kv", "tp"),
            P(),
            P("kv", "tp"),
            P("kv", "tp"),
            P("kv", "tp"),
            P("kv", "tp"),
            P("kv", "tp"),
            P("tp"),
            P(),
            P("tp", "kv"),
            P("tp"),
            P("tp", "kv"),
            P("kv", "tp"),
        ),
        out_specs=(P("kv", "tp"), P("kv", "tp")),
        check_vma=False,
    )
```

```python
import functools

import jax
import jax.numpy as jnp
from jax import lax
from jax.experimental import pallas as pl
from jax.experimental.pallas import tpu as pltpu
from jax.sharding import PartitionSpec as P

DK = 128
DV = 256

epsilon = 1e-06
decay_normalizer = 16.0

F32 = jnp.float32
BF16 = jnp.bfloat16
MESH = pl.DeviceIdType.MESH
CHUNKS = 2
SPLIT = 1
LATE = 1
ONES = 19
STORES = 8
VMEM_BYTES = 67043328


def remote(src, dst, send_sem, recv_sem, i, j):
    return pltpu.make_async_remote_copy(
        src_ref=src,
        dst_ref=dst,
        send_sem=send_sem,
        recv_sem=recv_sem,
        device_id={"kv": i, "tp": j},
        device_id_type=MESH,
    )


def dot(a, b):
    return jnp.dot(a, b, preferred_element_type=F32)


def inner_size(kv):
    size = 1
    while (size * 2) ** 2 <= kv:
        size = size * 2
    return size


def layer_kernel(
    kv, tp,
    h_in, ng_in, bias_in, hg_in, mg_in, wq, wk, wd_, wv, wg, old, wo, wu, wdn,
    out_ref, st_ref,
    h_ref, ng_ref, bias_ref, hg_ref, mg_ref, gains,
    vq, vk, vd_, vv, vg, vo, vu, vdn,
    xbuf, psnd, prcv, zsnd, zrcv, wsnd, wrcv, vsnd, vrcv, ssq, query, key, decay, value, head,
    mixed, mall, asend, arecv, rpart, rall, usend, urecv, xsend, xrecv, act, dsend, drecv, ssq2,
    insem, wsem, hr_sem, pr_sem, qr_sem, wr_sem, er_sem, mr_sem, ar_sem, rr_sem,
    ur_sem, xr_sem, cr_sem, dr_sem, one,
):
    i, j = lax.axis_index("kv"), lax.axis_index("tp")
    ny = inner_size(kv)
    nz = kv // ny
    z, y = i // ny, lax.rem(i, ny)
    ratio = kv // tp
    owner = i // ratio
    rows = h_ref.shape[0]
    eight = rows // 2
    columns = h_ref.shape[1]
    width = xbuf.shape[2]
    cw = vq.shape[1]
    pw = psnd.shape[4]
    heads = cw // DK
    core = lax.rem(j, 2)
    across = j // 2
    other = 1 - core
    partner = across * 2 + other
    (
        st_sem, hs_sem, fs_sem, fr_sem, ss_sem, sr_sem, ps_sem, qs_sem, ws_sem, es_sem,
        ms_sem, as_sem, rs_sem, ts_sem, tr_sem, us_sem, xs_sem, cs_sem, ds_sem,
    ) = [one.at[n] for n in range(ONES)]

    def take(ref, sem):
        remote(ref, ref, sem, sem, i, partner).wait_recv()

    def drain(ref, sem):
        remote(ref, ref, sem, sem, i, partner).wait_send()

    def send(src, dst, send_sem, recv_sem, a, b):
        remote(src, dst, send_sem, recv_sem, a, b).start()

    inputs = [
        pltpu.make_async_copy(src, dst, insem.at[n])
        for n, (src, dst) in enumerate(
            ((h_in, h_ref), (ng_in, ng_ref), (bias_in, bias_ref), (hg_in, hg_ref), (mg_in, mg_ref))
        )
    ]
    for copy in inputs:
        copy.start()
    barrier = pltpu.get_barrier_semaphore()

    def greet(a, b):
        pl.semaphore_signal(
            barrier, inc=1, device_id={"kv": a, "tp": b}, device_id_type=MESH
        )

    for s in range(kv):
        k = lax.rem(i + s, kv)
        if s:
            greet(k, owner)
            greet(k, j)
        else:
            pl.when(owner != j)(lambda: greet(i, owner))
    for a in range(ratio):
        for s in range(tp):
            k, t = j * ratio + a, lax.rem(j + s, tp)
            if s:
                greet(k, t)
            else:
                pl.when(k != i)(functools.partial(greet, k, t))
    for s in range(1, tp):
        greet(i, lax.rem(j + s, tp))

    loads = [
        pltpu.make_async_copy(w, v, wsem.at[n])
        for n, (w, v) in enumerate(
            ((wd_, vd_), (wk, vk), (wq, vq), (wv, vv), (wg, vg), (wo, vo), (wu, vu), (wdn, vdn))
        )
    ]
    load_state = pltpu.make_async_copy(old, st_ref, st_sem)
    for load in loads[:5]:
        load.start()
    load_state.start()
    for load in loads[5:]:
        load.start()

    for copy in inputs:
        copy.wait()
    hidden = h_ref[...].astype(F32)
    ssq[j] = jnp.broadcast_to(jnp.sum(hidden * hidden, axis=1, keepdims=True), (rows, 128))
    itself = jnp.where(owner == j, 1, 0)
    pl.semaphore_wait(barrier, 2 * (kv - itself) + (kv - 1) + (tp - 1))

    side = lax.rem(i, 2)
    for a in range(ratio):
        k = j * ratio + a
        for s in range(tp // 2):
            t = lax.rem(across + s, tp // 2) * 2 + side
            copy = remote(
                h_ref.at[:, pl.ds(a * width, width)], xbuf.at[i], hs_sem, hr_sem.at[i // 2], k, t
            )
            if s:
                copy.start()
            else:
                here = jnp.logical_and(k == i, t == j)
                pl.when(jnp.logical_not(here))(copy.start)

                @pl.when(here)
                def _():
                    xbuf[i] = h_ref[:, a * width : (a + 1) * width]

    for s in range(1, tp):
        send(ssq.at[j], ssq.at[j], ss_sem, sr_sem, i, lax.rem(j + s, tp))

    gains[...] = ng_ref[...].astype(F32).reshape(1, kv * width)
    gain = gains[:, pl.ds(pl.multiple_of(i * width, 128), width)]
    for s in range(kv // 2):
        m = lax.rem(i // 2 + s, kv // 2)
        k = 2 * m + core
        if s:
            take(xbuf.at[k], hr_sem.at[m])
        else:
            pl.when(jnp.logical_or(owner != j, k != i))(lambda: take(xbuf.at[k], hr_sem.at[m]))
        send(xbuf.at[k], xbuf.at[k], fs_sem, fr_sem, i, partner)
    take(xbuf.at[pl.ds(0, kv // 2)], fr_sem)
    x = (xbuf[...].reshape(kv * rows, width).astype(F32) * gain).astype(BF16)

    pieces = []
    for n, v in enumerate((vd_, vk, vq, vv, vg)):
        for low in range(0, v.shape[1], pw):
            pieces.append((n, v, low))
    late = len(pieces) - wsnd.shape[0]
    ready = set()

    def product(c):
        n, v, low = pieces[c]
        if n not in ready:
            loads[n].wait()
            ready.add(n)
        return dot(x, v[:, low : low + pw]).astype(BF16)

    def first_z(c):
        part, e = product(c), c - late
        for zz in range(nz):
            for yy in range(ny):
                at = (zz * ny + yy) * rows
                wsnd[e, zz, yy] = part[at : at + rows]
        for s in range(1, nz):
            zz = lax.rem(z + s, nz)
            send(wsnd.at[e, zz], wrcv.at[e, s - 1], ws_sem, wr_sem.at[e], zz * ny + y, j)

    def first_y(c):
        part = product(c)
        for zz in range(nz):
            for yy in range(ny):
                at = (zz * ny + yy) * rows
                psnd[c, yy, zz] = part[at : at + rows]
        for s in range(1, ny):
            yy = lax.rem(y + s, ny)
            send(psnd.at[c, yy], prcv.at[c, s - 1], ps_sem, pr_sem.at[c], z * ny + yy, j)

    def then_y(c):
        e = c - late
        take(wrcv.at[e], wr_sem.at[e])
        acc = wsnd[e, z].astype(F32)
        for s in range(1, nz):
            acc = acc + wrcv[e, s - 1].astype(F32)
        vsnd[e] = acc.astype(BF16)
        for s in range(1, ny):
            yy = lax.rem(y + s, ny)
            send(vsnd.at[e, yy], vrcv.at[e, s - 1], es_sem, er_sem.at[e], z * ny + yy, j)

    def then_z(c):
        take(prcv.at[c], pr_sem.at[c])
        acc = psnd[c, y].astype(F32)
        for s in range(1, ny):
            acc = acc + prcv[c, s - 1].astype(F32)
        zsnd[c] = acc.astype(BF16)
        for s in range(1, nz):
            zz = lax.rem(z + s, nz)
            send(zsnd.at[c, zz], zrcv.at[c, s - 1], qs_sem, qr_sem.at[c], zz * ny + y, j)

    def reduced_piece(c):
        if c >= late:
            e = c - late
            take(vrcv.at[e], er_sem.at[e])
            acc = vsnd[e, y].astype(F32)
            for s in range(1, ny):
                acc = acc + vrcv[e, s - 1].astype(F32)
        else:
            take(zrcv.at[c], qr_sem.at[c])
            acc = zsnd[c, z].astype(F32)
            for s in range(1, nz):
                acc = acc + zrcv[c, s - 1].astype(F32)
        return (acc * scale).astype(BF16).astype(F32)

    def reduced(c):
        per = cw // pw
        return jnp.concatenate([reduced_piece(c * per + m) for m in range(per)], axis=1)

    def head_slices(h):
        narrow = pl.ds(pl.multiple_of(h * DK, DK), DK)
        wide = pl.ds(pl.multiple_of(h * DV, DV), DV)
        return narrow, wide

    def state_slice(h, c):
        return pl.ds(pl.multiple_of(h * (DK * DV) + c * DV, DV), DV)

    def read_state(low, high):
        @pl.loop(low, high)
        def _(h):
            narrow, wide = head_slices(h)
            q = query[:, narrow] * decay[:, narrow]
            acc = jnp.zeros((rows, DV), F32)
            for c in range(DK):
                acc = acc + q[:, c : c + 1] * st_ref[:, state_slice(h, c)]
            head[:, wide] = acc

    def write_state(low, high):
        @pl.loop(low, high)
        def _(h):
            narrow, wide = head_slices(h)
            k, d = key[:, narrow], decay[:, narrow]
            v = value[:, wide]
            for c in range(DK):
                at = state_slice(h, c)
                st_ref[:, at] = d[:, c : c + 1] * st_ref[:, at] + k[:, c : c + 1] * v

    for c in range(late, len(pieces)):
        first_z(c)
    for c in range(late):
        first_y(c)
    early = late - 1
    for c in range(early):
        then_z(c)
        if c == late // 2:
            for e in range(late, len(pieces)):
                then_y(e)
    take(ssq.at[pl.ds(0, tp - 1)], sr_sem)
    total = ssq[0]
    for s in range(1, tp):
        total = total + ssq[s]
    scale = lax.rsqrt(total[:, :1] / (kv * width) + epsilon)

    pre = reduced(0) + bias_ref[...]
    log_decay = jnp.minimum(pre, 0.0) - jnp.log1p(jnp.exp(-jnp.abs(pre)))
    decay[...] = jnp.exp(log_decay / decay_normalizer)
    key[...] = reduced(1)
    query[...] = reduced(2) * DK ** (-0.5)
    load_state.wait()
    read_state(0, heads // 2)
    for c in range(early, late):
        then_z(c)
    read_state(heads // 2, heads)
    for c in range(3, 5):
        value[:, (c - 3) * cw : (c - 2) * cw] = reduced(c)
    head_gain = hg_ref[...].astype(F32).reshape(1, DV)
    for h in range(heads):
        at = slice(h * DK, (h + 1) * DK)
        weight = jnp.sum(query[:, at] * key[:, at], axis=1, keepdims=True)
        at = slice(h * DV, (h + 1) * DV)
        acc = head[:, at] + weight * value[:, at]
        acc = acc * lax.rsqrt(jnp.mean(acc * acc, axis=1, keepdims=True) + epsilon)
        head[:, at] = acc * head_gain

    for c in range(5, 7):
        at = slice((c - 5) * cw, (c - 4) * cw)
        both = head[:, at] * jax.nn.silu(reduced(c))
        for p in range(2):
            mixed[p, :, at] = both[p * eight : (p + 1) * eight].astype(BF16)

    for p in range(2):
        for s in range(1, kv):
            k = lax.rem(i + s, kv)
            send(mixed.at[p], mall.at[p, i], ms_sem, mr_sem.at[p], k, j)
    for p in range(2):
        mall[p, i] = mixed[p]
    write_state(0, heads // 4)

    loads[5].wait()
    tokens = kv * eight
    for p in range(2):
        take(mall.at[p, pl.ds(0, kv - 1)], mr_sem.at[p])
        every = mall[p].astype(F32).reshape(tokens, mall.shape[3]).astype(BF16)
        asend[p] = dot(every, vo[...]).astype(BF16).reshape(asend.shape[1:])
        for s in range(1, tp):
            t = lax.rem(j + s, tp)
            send(asend.at[p, t], arecv.at[p, s - 1], as_sem, ar_sem.at[p], i, t)
    slot = lax.rem(i, ratio)
    place = slot * tp + j
    mine = xbuf[pl.ds(j * ratio, ratio)].astype(F32)
    for p in range(2):
        take(arecv.at[p], ar_sem.at[p])
        attn = asend[p, j].astype(F32)
        for s in range(1, tp):
            attn = attn + arecv[p, s - 1].astype(F32)
        part = mine[:, p * eight : (p + 1) * eight].reshape(ratio * eight, width)
        rpart[p] = (part + attn.astype(BF16).astype(F32)).astype(BF16)
        for s in range(kv):
            k = lax.rem(i + s, kv)
            copy = remote(rpart.at[p], rall.at[p, place], rs_sem, rr_sem.at[p], k, owner)
            if s:
                copy.start()
            else:
                pl.when(owner != j)(copy.start)

    @pl.when(owner == j)
    def _():
        for p in range(2):
            rall[p, place] = rpart[p]

    write_state(heads // 4, heads // 2)
    loads[6].wait()
    mlp_gain = mg_ref[...].astype(F32).reshape(1, columns)

    def gathered(p):
        pl.when(owner == j)(lambda: take(rall.at[p, pl.ds(0, kv - 1)], rr_sem.at[p]))
        pl.when(owner != j)(lambda: take(rall.at[p], rr_sem.at[p]))
        return jnp.concatenate(
            [
                (
                    rall[p, a * tp : (a + 1) * tp].reshape(tokens, width).astype(F32)
                    * mlp_gain[:, a * width : (a + 1) * width]
                ).astype(BF16)
                for a in range(ratio)
            ],
            axis=1,
        )

    def own(p, a):
        group = rall[p, a * tp + owner].astype(F32)
        value = group[:eight]
        for m in range(1, ratio):
            value = jnp.where(slot == m, group[m * eight : (m + 1) * eight], value)
        return value

    half = vu.shape[1] // 2
    chunks = usend.shape[1]
    piece = half // chunks

    def columns_of(h, c):
        return pl.ds(pl.multiple_of(h * half + c * piece, 128), piece)

    def up(p, x):
        def give(c):
            usend[p, c] = dot(x, vu[:, columns_of(other, c)]).astype(BF16)
            send(usend.at[p, c], urecv.at[p, c], us_sem, ur_sem.at[p, c], i, partner)

        give(0)
        for c in range(chunks):
            if c + 1 < chunks:
                give(c + 1)
            mine = dot(x, vu[:, columns_of(core, c)])
            take(urecv.at[p, c], ur_sem.at[p, c])
            xsend[p, c] = (mine + urecv[p, c].astype(F32)).astype(BF16)
            for s in range(1, tp // 2):
                to = lax.rem(across + s, tp // 2)
                send(
                    xsend.at[p, c], xrecv.at[p, c, s - 1], xs_sem, xr_sem.at[p, c],
                    i, to * 2 + core,
                )

    def down(p):
        acc = None
        for c in range(chunks):
            take(xrecv.at[p, c], xr_sem.at[p, c])
            total = xsend[p, c].astype(F32)
            for s in range(1, tp // 2):
                total = total + xrecv[p, c, s - 1].astype(F32)
            act[p, 0, c] = jnp.square(jnp.maximum(total, 0.0)).astype(BF16)
            send(act.at[p, 0, c], act.at[p, 1, c], cs_sem, cr_sem.at[p, c], i, partner)
            term = dot(act[p, 0, c], vdn[columns_of(core, c), :])
            acc = term if acc is None else acc + term
        for c in range(chunks):
            take(act.at[p, 1, c], cr_sem.at[p, c])
            acc = acc + dot(act[p, 1, c], vdn[columns_of(other, c), :])
        dsend[p] = acc.reshape(kv, eight, columns).astype(BF16)
        for s in range(1, kv):
            k = lax.rem(i + s, kv)
            send(dsend.at[p, k], drecv.at[p, s - 1], ds_sem, dr_sem.at[p], k, j)

    x0 = gathered(0)
    up(0, x0)
    x1 = gathered(1)
    squares = []
    for p in range(2):
        terms = [own(p, a) for a in range(ratio)]
        squares.append(sum(jnp.sum(term * term, axis=1, keepdims=True) for term in terms))
    squares = jnp.concatenate(squares, axis=0)
    ssq2[j] = jnp.broadcast_to(squares, (rows, 128))
    for s in range(1, tp):
        send(ssq2.at[j], ssq2.at[j], ts_sem, tr_sem, i, lax.rem(j + s, tp))
    up(1, x1)
    loads[7].wait()
    down(0)
    down(1)
    write_state(heads // 2, heads)

    take(ssq2.at[pl.ds(0, tp - 1)], tr_sem)
    squares = ssq2[0]
    for s in range(1, tp):
        squares = squares + ssq2[s]
    scale2 = lax.rsqrt(squares[:, :1] / (columns * tp) + epsilon)
    lines = []
    for p in range(2):
        take(drecv.at[p], dr_sem.at[p])
        acc = dsend[p, i].astype(F32)
        for s in range(1, kv):
            acc = acc + drecv[p, s - 1].astype(F32)
        part = scale2[p * eight : (p + 1) * eight]
        acc = (acc * (part * part)).astype(BF16).astype(F32)
        base = jnp.concatenate([own(p, a) for a in range(ratio)], axis=1)
        lines.append(base + acc)
    out_ref[...] = jnp.concatenate(lines, axis=0).astype(BF16)

    here = jnp.logical_and(owner == j, side == core)
    pl.when(here)(lambda: drain(xbuf.at[pl.ds(0, kv // 2 - 1)], hs_sem))
    pl.when(jnp.logical_not(here))(lambda: drain(xbuf.at[pl.ds(0, kv // 2)], hs_sem))
    drain(xbuf.at[pl.ds(0, kv // 2)], fs_sem)
    drain(ssq.at[pl.ds(0, tp - 1)], ss_sem)
    drain(prcv, ps_sem)
    drain(zrcv, qs_sem)
    drain(wrcv, ws_sem)
    drain(vrcv, es_sem)
    drain(mall.at[:, pl.ds(0, kv - 1)], ms_sem)
    drain(arecv, as_sem)
    pl.when(owner == j)(lambda: drain(rall.at[:, pl.ds(0, kv - 1)], rs_sem))
    pl.when(owner != j)(lambda: drain(rall, rs_sem))
    drain(ssq2.at[pl.ds(0, tp - 1)], ts_sem)
    drain(usend, us_sem)
    drain(xrecv, xs_sem)
    drain(act.at[:, 0], cs_sem)
    drain(drecv, ds_sem)


def layer(
    kv, tp, hidden_rows, carried, norm_gain, weights, decay_bias, head_gain, w_out, mlp_gain,
    w_up, w_down,
):
    rows, columns = hidden_rows.shape
    width = w_out.shape[1]
    ratio = kv // tp
    ny = inner_size(kv)
    nz = kv // ny
    cw = weights[0].shape[1]
    wide = weights[3].shape[1]
    pw = cw // SPLIT
    pieces = sum(w.shape[1] for w in weights) // pw
    late = LATE
    half = w_up.shape[1] // 2
    eight = rows // 2
    tokens = kv * eight
    chunks = max(1, min(CHUNKS, half // 128))
    piece = half // chunks
    limit = VMEM_BYTES - 4 * carried.size - 128 * 1024
    vmem = pl.BlockSpec(memory_space=pltpu.VMEM)
    hbm = pl.BlockSpec(memory_space=pltpu.HBM)
    dma = pltpu.SemaphoreType.DMA
    wq, wk, wd_, wv, wg = weights
    bias = decay_bias.reshape(1, -1)
    return pl.pallas_call(
        functools.partial(layer_kernel, kv, tp),
        out_shape=[
            pltpu.VMEM((rows, columns), BF16),
            pltpu.VMEM(carried.shape, F32),
        ],
        in_specs=[hbm] * 14,
        out_specs=[vmem, vmem],
        scratch_shapes=[
            pltpu.VMEM(a.shape, a.dtype)
            for a in (hidden_rows, norm_gain, bias, head_gain, mlp_gain)
        ]
        + [pltpu.VMEM((1, norm_gain.shape[0]), F32)]
        + [
            pltpu.VMEM(w.shape, BF16) for w in (wq, wk, wd_, wv, wg, w_out, w_up, w_down)
        ]
        + [
            pltpu.VMEM((kv, rows, width), BF16),
            pltpu.VMEM((pieces - late, ny, nz, rows, pw), BF16),
            pltpu.VMEM((pieces - late, ny - 1, nz, rows, pw), BF16),
            pltpu.VMEM((pieces - late, nz, rows, pw), BF16),
            pltpu.VMEM((pieces - late, nz - 1, rows, pw), BF16),
            pltpu.VMEM((late, nz, ny, rows, pw), BF16),
            pltpu.VMEM((late, nz - 1, ny, rows, pw), BF16),
            pltpu.VMEM((late, ny, rows, pw), BF16),
            pltpu.VMEM((late, ny - 1, rows, pw), BF16),
            pltpu.VMEM((tp, rows, 128), F32),
            pltpu.VMEM((rows, cw), F32),
            pltpu.VMEM((rows, cw), F32),
            pltpu.VMEM((rows, cw), F32),
            pltpu.VMEM((rows, wide), F32),
            pltpu.VMEM((rows, wide), F32),
            pltpu.VMEM((2, eight, wide), BF16),
            pltpu.VMEM((2, kv, eight, wide), BF16),
            pltpu.VMEM((2, tp, ratio * eight, width), BF16),
            pltpu.VMEM((2, tp - 1, ratio * eight, width), BF16),
            pltpu.VMEM((2, ratio * eight, width), BF16),
            pltpu.VMEM((2, kv, ratio * eight, width), BF16),
            pltpu.VMEM((2, chunks, tokens, piece), BF16),
            pltpu.VMEM((2, chunks, tokens, piece), BF16),
            pltpu.VMEM((2, chunks, tokens, piece), BF16),
            pltpu.VMEM((2, chunks, tp // 2 - 1, tokens, piece), BF16),
            pltpu.VMEM((2, 2, chunks, tokens, piece), BF16),
            pltpu.VMEM((2, kv, eight, columns), BF16),
            pltpu.VMEM((2, kv - 1, eight, columns), BF16),
            pltpu.VMEM((tp, rows, 128), F32),
            dma((5,)),
            dma((8,)),
            dma((kv // 2,)),
            dma((pieces - late,)),
            dma((pieces - late,)),
            dma((late,)),
            dma((late,)),
            dma((2,)),
            dma((2,)),
            dma((2,)),
            dma((2, chunks)),
            dma((2, chunks)),
            dma((2, chunks)),
            dma((2,)),
            dma((ONES,)),
        ],
        compiler_params=pltpu.CompilerParams(
            has_side_effects=True, collective_id=0, vmem_limit_bytes=limit
        ),
        name="layer",
    )(
        hidden_rows, norm_gain, bias, head_gain, mlp_gain, wq, wk, wd_, wv, wg, carried,
        w_out, w_up, w_down,
    )


def store_kernel(parts, new_in, rows_in, new_out, rows_out, sems):
    size = new_in.shape[1] // parts
    copies = [pltpu.make_async_copy(rows_in, rows_out, sems.at[parts])]
    for n in range(parts):
        at = pl.ds(n * size, size)
        copies.append(pltpu.make_async_copy(new_in.at[:, at], new_out.at[:, at], sems.at[n]))
    for copy in copies:
        copy.start()
    for copy in copies:
        copy.wait()


def store(updated_rows, new_state):
    parts = STORES
    vmem = pl.BlockSpec(memory_space=pltpu.VMEM)
    hbm = pl.BlockSpec(memory_space=pltpu.HBM)
    return pl.pallas_call(
        functools.partial(store_kernel, parts),
        out_shape=[
            jax.ShapeDtypeStruct(new_state.shape, new_state.dtype),
            jax.ShapeDtypeStruct(updated_rows.shape, updated_rows.dtype),
        ],
        in_specs=[vmem, vmem],
        out_specs=[hbm, hbm],
        scratch_shapes=[pltpu.SemaphoreType.DMA((parts + 1,))],
        compiler_params=pltpu.CompilerParams(vmem_limit_bytes=1024 * 1024),
        name="store",
    )(new_state, updated_rows)


def body(
    kv,
    tp,
    hidden_rows,
    carried_state,
    norm_gain,
    w_query,
    w_key,
    w_decay,
    w_value,
    w_gate,
    decay_bias,
    head_gain,
    w_out,
    mlp_gain,
    w_up,
    w_down,
):
    updated_rows, new_state = layer(
        kv, tp, hidden_rows, carried_state, norm_gain,
        (w_query, w_key, w_decay, w_value, w_gate), decay_bias, head_gain, w_out, mlp_gain,
        w_up, w_down,
    )
    new_state, updated_rows = store(updated_rows, new_state)
    return (updated_rows, new_state)


def solution(mesh):
    return jax.shard_map(
        functools.partial(body, mesh.shape["kv"], mesh.shape["tp"]),
        mesh=mesh,
        in_specs=(
            P("kv", "tp"),
            P("kv", "tp"),
            P(),
            P("kv", "tp"),
            P("kv", "tp"),
            P("kv", "tp"),
            P("kv", "tp"),
            P("kv", "tp"),
            P("tp"),
            P(),
            P("tp", "kv"),
            P("tp"),
            P("tp", "kv"),
            P("kv", "tp"),
        ),
        out_specs=(P("kv", "tp"), P("kv", "tp")),
        check_vma=False,
    )
```

```python
import functools

import jax
import jax.numpy as jnp
from jax import lax
from jax.experimental import pallas as pl
from jax.experimental.pallas import tpu as pltpu
from jax.sharding import PartitionSpec as P

DK = 128
DV = 256

epsilon = 1e-06
decay_normalizer = 16.0

F32 = jnp.float32
BF16 = jnp.bfloat16
MESH = pl.DeviceIdType.MESH
CHUNKS = 2
SPLIT = 1
LATE = 1
ONES = 19
STORES = 8
VMEM_BYTES = 67043328


def remote(src, dst, send_sem, recv_sem, i, j):
    return pltpu.make_async_remote_copy(
        src_ref=src,
        dst_ref=dst,
        send_sem=send_sem,
        recv_sem=recv_sem,
        device_id={"kv": i, "tp": j},
        device_id_type=MESH,
    )


def dot(a, b):
    return jnp.dot(a, b, preferred_element_type=F32)


def inner_size(kv):
    size = 1
    while (size * 2) ** 2 <= kv:
        size = size * 2
    return size


def layer_kernel(
    kv, tp,
    h_in, ng_in, bias_in, hg_in, mg_in, wq, wk, wd_, wv, wg, old, wo, wu, wdn,
    out_ref, st_ref,
    h_ref, ng_ref, bias_ref, hg_ref, mg_ref, gains,
    vq, vk, vd_, vv, vg, vo, vu, vdn,
    xbuf, psnd, prcv, zsnd, zrcv, wsnd, wrcv, vsnd, vrcv, ssq, query, key, decay, value, head,
    mixed, mall, asend, arecv, rpart, rall, usend, urecv, xsend, xrecv, act, dsend, drecv, ssq2,
    insem, wsem, hr_sem, pr_sem, qr_sem, wr_sem, er_sem, mr_sem, ar_sem, rr_sem,
    ur_sem, xr_sem, cr_sem, dr_sem, one,
):
    i, j = lax.axis_index("kv"), lax.axis_index("tp")
    ny = inner_size(kv)
    nz = kv // ny
    z, y = i // ny, lax.rem(i, ny)
    ratio = kv // tp
    owner = i // ratio
    rows = h_ref.shape[0]
    eight = rows // 2
    columns = h_ref.shape[1]
    width = xbuf.shape[2]
    cw = vq.shape[1]
    pw = psnd.shape[4]
    heads = cw // DK
    core = lax.rem(j, 2)
    across = j // 2
    other = 1 - core
    partner = across * 2 + other
    (
        st_sem, hs_sem, fs_sem, fr_sem, ss_sem, sr_sem, ps_sem, qs_sem, ws_sem, es_sem,
        ms_sem, as_sem, rs_sem, ts_sem, tr_sem, us_sem, xs_sem, cs_sem, ds_sem,
    ) = [one.at[n] for n in range(ONES)]

    def take(ref, sem):
        remote(ref, ref, sem, sem, i, partner).wait_recv()

    def drain(ref, sem):
        remote(ref, ref, sem, sem, i, partner).wait_send()

    def send(src, dst, send_sem, recv_sem, a, b):
        remote(src, dst, send_sem, recv_sem, a, b).start()

    inputs = [
        pltpu.make_async_copy(src, dst, insem.at[n])
        for n, (src, dst) in enumerate(
            ((h_in, h_ref), (ng_in, ng_ref), (bias_in, bias_ref), (hg_in, hg_ref), (mg_in, mg_ref))
        )
    ]
    for copy in inputs:
        copy.start()
    barrier = pltpu.get_barrier_semaphore()

    def greet(a, b):
        pl.semaphore_signal(
            barrier, inc=1, device_id={"kv": a, "tp": b}, device_id_type=MESH
        )

    for s in range(kv):
        k = lax.rem(i + s, kv)
        if s:
            greet(k, owner)
            greet(k, j)
        else:
            pl.when(owner != j)(lambda: greet(i, owner))
    for a in range(ratio):
        for s in range(tp):
            k, t = j * ratio + a, lax.rem(j + s, tp)
            if s:
                greet(k, t)
            else:
                pl.when(k != i)(functools.partial(greet, k, t))
    for s in range(1, tp):
        greet(i, lax.rem(j + s, tp))

    loads = [
        pltpu.make_async_copy(w, v, wsem.at[n])
        for n, (w, v) in enumerate(
            ((wd_, vd_), (wk, vk), (wq, vq), (wv, vv), (wg, vg), (wo, vo), (wu, vu), (wdn, vdn))
        )
    ]
    load_state = pltpu.make_async_copy(old, st_ref, st_sem)
    for load in loads[:5]:
        load.start()
    load_state.start()
    for load in loads[5:]:
        load.start()

    for copy in inputs:
        copy.wait()
    hidden = h_ref[...].astype(F32)
    ssq[j] = jnp.broadcast_to(jnp.sum(hidden * hidden, axis=1, keepdims=True), (rows, 128))
    itself = jnp.where(owner == j, 1, 0)
    pl.semaphore_wait(barrier, 2 * (kv - itself) + (kv - 1) + (tp - 1))

    side = lax.rem(i, 2)
    for a in range(ratio):
        k = j * ratio + a
        for s in range(tp // 2):
            t = lax.rem(across + s, tp // 2) * 2 + side
            copy = remote(
                h_ref.at[:, pl.ds(a * width, width)], xbuf.at[i], hs_sem, hr_sem.at[i // 2], k, t
            )
            if s:
                copy.start()
            else:
                here = jnp.logical_and(k == i, t == j)
                pl.when(jnp.logical_not(here))(copy.start)

                @pl.when(here)
                def _():
                    xbuf[i] = h_ref[:, a * width : (a + 1) * width]

    for s in range(1, tp):
        send(ssq.at[j], ssq.at[j], ss_sem, sr_sem, i, lax.rem(j + s, tp))

    gains[...] = ng_ref[...].astype(F32).reshape(1, kv * width)
    gain = gains[:, pl.ds(pl.multiple_of(i * width, 128), width)]
    for s in range(kv // 2):
        m = lax.rem(i // 2 + s, kv // 2)
        k = 2 * m + core
        if s:
            take(xbuf.at[k], hr_sem.at[m])
        else:
            pl.when(jnp.logical_or(owner != j, k != i))(lambda: take(xbuf.at[k], hr_sem.at[m]))
        send(xbuf.at[k], xbuf.at[k], fs_sem, fr_sem, i, partner)
    take(xbuf.at[pl.ds(0, kv // 2)], fr_sem)
    x = (xbuf[...].reshape(kv * rows, width).astype(F32) * gain).astype(BF16)

    pieces = []
    for n, v in enumerate((vd_, vk, vq, vv, vg)):
        for low in range(0, v.shape[1], pw):
            pieces.append((n, v, low))
    late = len(pieces) - wsnd.shape[0]
    ready = set()

    def product(c):
        n, v, low = pieces[c]
        if n not in ready:
            loads[n].wait()
            ready.add(n)
        return dot(x, v[:, low : low + pw]).astype(BF16)

    def first_z(c):
        part, e = product(c), c - late
        for zz in range(nz):
            for yy in range(ny):
                at = (zz * ny + yy) * rows
                wsnd[e, zz, yy] = part[at : at + rows]
        for s in range(1, nz):
            zz = lax.rem(z + s, nz)
            send(wsnd.at[e, zz], wrcv.at[e, s - 1], ws_sem, wr_sem.at[e], zz * ny + y, j)

    def first_y(c):
        part = product(c)
        for zz in range(nz):
            for yy in range(ny):
                at = (zz * ny + yy) * rows
                psnd[c, yy, zz] = part[at : at + rows]
        for s in range(1, ny):
            yy = lax.rem(y + s, ny)
            send(psnd.at[c, yy], prcv.at[c, s - 1], ps_sem, pr_sem.at[c], z * ny + yy, j)

    def then_y(c):
        e = c - late
        take(wrcv.at[e], wr_sem.at[e])
        acc = wsnd[e, z].astype(F32)
        for s in range(1, nz):
            acc = acc + wrcv[e, s - 1].astype(F32)
        vsnd[e] = acc.astype(BF16)
        for s in range(1, ny):
            yy = lax.rem(y + s, ny)
            send(vsnd.at[e, yy], vrcv.at[e, s - 1], es_sem, er_sem.at[e], z * ny + yy, j)

    def then_z(c):
        take(prcv.at[c], pr_sem.at[c])
        acc = psnd[c, y].astype(F32)
        for s in range(1, ny):
            acc = acc + prcv[c, s - 1].astype(F32)
        zsnd[c] = acc.astype(BF16)
        for s in range(1, nz):
            zz = lax.rem(z + s, nz)
            send(zsnd.at[c, zz], zrcv.at[c, s - 1], qs_sem, qr_sem.at[c], zz * ny + y, j)

    def reduced_piece(c):
        if c >= late:
            e = c - late
            take(vrcv.at[e], er_sem.at[e])
            acc = vsnd[e, y].astype(F32)
            for s in range(1, ny):
                acc = acc + vrcv[e, s - 1].astype(F32)
        else:
            take(zrcv.at[c], qr_sem.at[c])
            acc = zsnd[c, z].astype(F32)
            for s in range(1, nz):
                acc = acc + zrcv[c, s - 1].astype(F32)
        return (acc * scale).astype(BF16).astype(F32)

    def reduced(c):
        per = cw // pw
        return jnp.concatenate([reduced_piece(c * per + m) for m in range(per)], axis=1)

    def head_slices(h):
        narrow = pl.ds(pl.multiple_of(h * DK, DK), DK)
        wide = pl.ds(pl.multiple_of(h * DV, DV), DV)
        return narrow, wide

    def state_slice(h, c):
        return pl.ds(pl.multiple_of(h * (DK * DV) + c * DV, DV), DV)

    def read_state(low, high):
        @pl.loop(low, high)
        def _(h):
            narrow, wide = head_slices(h)
            q = query[:, narrow] * decay[:, narrow]
            acc = jnp.zeros((rows, DV), F32)
            for c in range(DK):
                acc = acc + q[:, c : c + 1] * st_ref[:, state_slice(h, c)]
            head[:, wide] = acc

    def write_state(low, high):
        @pl.loop(low, high)
        def _(h):
            narrow, wide = head_slices(h)
            k, d = key[:, narrow], decay[:, narrow]
            v = value[:, wide]
            for c in range(DK):
                at = state_slice(h, c)
                st_ref[:, at] = d[:, c : c + 1] * st_ref[:, at] + k[:, c : c + 1] * v

    first_y(0)
    for c in range(late, len(pieces)):
        first_z(c)
    for c in range(1, late):
        first_y(c)
    for c in range(late):
        if c == late - 1:
            for e in range(late, len(pieces)):
                then_y(e)
        then_z(c)
    take(ssq.at[pl.ds(0, tp - 1)], sr_sem)
    total = ssq[0]
    for s in range(1, tp):
        total = total + ssq[s]
    scale = lax.rsqrt(total[:, :1] / (kv * width) + epsilon)

    pre = reduced(0) + bias_ref[...]
    log_decay = jnp.minimum(pre, 0.0) - jnp.log1p(jnp.exp(-jnp.abs(pre)))
    decay[...] = jnp.exp(log_decay / decay_normalizer)
    key[...] = reduced(1)
    query[...] = reduced(2) * DK ** (-0.5)
    load_state.wait()
    read_state(0, heads)
    for c in range(3, 5):
        value[:, (c - 3) * cw : (c - 2) * cw] = reduced(c)
    head_gain = hg_ref[...].astype(F32).reshape(1, DV)
    for h in range(heads):
        at = slice(h * DK, (h + 1) * DK)
        weight = jnp.sum(query[:, at] * key[:, at], axis=1, keepdims=True)
        at = slice(h * DV, (h + 1) * DV)
        acc = head[:, at] + weight * value[:, at]
        acc = acc * lax.rsqrt(jnp.mean(acc * acc, axis=1, keepdims=True) + epsilon)
        head[:, at] = acc * head_gain

    for c in range(5, 7):
        at = slice((c - 5) * cw, (c - 4) * cw)
        both = head[:, at] * jax.nn.silu(reduced(c))
        for p in range(2):
            mixed[p, :, at] = both[p * eight : (p + 1) * eight].astype(BF16)

    for p in range(2):
        for s in range(1, kv):
            k = lax.rem(i + s, kv)
            send(mixed.at[p], mall.at[p, i], ms_sem, mr_sem.at[p], k, j)
    for p in range(2):
        mall[p, i] = mixed[p]
    write_state(0, heads // 2)

    loads[5].wait()
    tokens = kv * eight
    for p in range(2):
        take(mall.at[p, pl.ds(0, kv - 1)], mr_sem.at[p])
        every = mall[p].astype(F32).reshape(tokens, mall.shape[3]).astype(BF16)
        asend[p] = dot(every, vo[...]).astype(BF16).reshape(asend.shape[1:])
        for s in range(1, tp):
            t = lax.rem(j + s, tp)
            send(asend.at[p, t], arecv.at[p, s - 1], as_sem, ar_sem.at[p], i, t)
    slot = lax.rem(i, ratio)
    place = slot * tp + j
    mine = xbuf[pl.ds(j * ratio, ratio)].astype(F32)
    for p in range(2):
        take(arecv.at[p], ar_sem.at[p])
        attn = asend[p, j].astype(F32)
        for s in range(1, tp):
            attn = attn + arecv[p, s - 1].astype(F32)
        part = mine[:, p * eight : (p + 1) * eight].reshape(ratio * eight, width)
        rpart[p] = (part + attn.astype(BF16).astype(F32)).astype(BF16)
        for s in range(kv):
            k = lax.rem(i + s, kv)
            copy = remote(rpart.at[p], rall.at[p, place], rs_sem, rr_sem.at[p], k, owner)
            if s:
                copy.start()
            else:
                pl.when(owner != j)(copy.start)

    @pl.when(owner == j)
    def _():
        for p in range(2):
            rall[p, place] = rpart[p]

    loads[6].wait()
    mlp_gain = mg_ref[...].astype(F32).reshape(1, columns)

    def gathered(p):
        pl.when(owner == j)(lambda: take(rall.at[p, pl.ds(0, kv - 1)], rr_sem.at[p]))
        pl.when(owner != j)(lambda: take(rall.at[p], rr_sem.at[p]))
        return jnp.concatenate(
            [
                (
                    rall[p, a * tp : (a + 1) * tp].reshape(tokens, width).astype(F32)
                    * mlp_gain[:, a * width : (a + 1) * width]
                ).astype(BF16)
                for a in range(ratio)
            ],
            axis=1,
        )

    def own(p, a):
        group = rall[p, a * tp + owner].astype(F32)
        value = group[:eight]
        for m in range(1, ratio):
            value = jnp.where(slot == m, group[m * eight : (m + 1) * eight], value)
        return value

    half = vu.shape[1] // 2
    chunks = usend.shape[1]
    piece = half // chunks

    def columns_of(h, c):
        return pl.ds(pl.multiple_of(h * half + c * piece, 128), piece)

    def up(p, x):
        def give(c):
            usend[p, c] = dot(x, vu[:, columns_of(other, c)]).astype(BF16)
            send(usend.at[p, c], urecv.at[p, c], us_sem, ur_sem.at[p, c], i, partner)

        give(0)
        for c in range(chunks):
            if c + 1 < chunks:
                give(c + 1)
            mine = dot(x, vu[:, columns_of(core, c)])
            take(urecv.at[p, c], ur_sem.at[p, c])
            xsend[p, c] = (mine + urecv[p, c].astype(F32)).astype(BF16)
            for s in range(1, tp // 2):
                to = lax.rem(across + s, tp // 2)
                send(
                    xsend.at[p, c], xrecv.at[p, c, s - 1], xs_sem, xr_sem.at[p, c],
                    i, to * 2 + core,
                )

    def down(p):
        acc = None
        for c in range(chunks):
            take(xrecv.at[p, c], xr_sem.at[p, c])
            total = xsend[p, c].astype(F32)
            for s in range(1, tp // 2):
                total = total + xrecv[p, c, s - 1].astype(F32)
            act[p, 0, c] = jnp.square(jnp.maximum(total, 0.0)).astype(BF16)
            send(act.at[p, 0, c], act.at[p, 1, c], cs_sem, cr_sem.at[p, c], i, partner)
            term = dot(act[p, 0, c], vdn[columns_of(core, c), :])
            acc = term if acc is None else acc + term
        for c in range(chunks):
            take(act.at[p, 1, c], cr_sem.at[p, c])
            acc = acc + dot(act[p, 1, c], vdn[columns_of(other, c), :])
        dsend[p] = acc.reshape(kv, eight, columns).astype(BF16)
        for s in range(1, kv):
            k = lax.rem(i + s, kv)
            send(dsend.at[p, k], drecv.at[p, s - 1], ds_sem, dr_sem.at[p], k, j)

    x0 = gathered(0)
    up(0, x0)
    x1 = gathered(1)
    up(1, x1)
    squares = []
    for p in range(2):
        terms = [own(p, a) for a in range(ratio)]
        squares.append(sum(jnp.sum(term * term, axis=1, keepdims=True) for term in terms))
    squares = jnp.concatenate(squares, axis=0)
    ssq2[j] = jnp.broadcast_to(squares, (rows, 128))
    for s in range(1, tp):
        send(ssq2.at[j], ssq2.at[j], ts_sem, tr_sem, i, lax.rem(j + s, tp))
    loads[7].wait()
    down(0)
    down(1)
    write_state(heads // 2, heads)

    take(ssq2.at[pl.ds(0, tp - 1)], tr_sem)
    squares = ssq2[0]
    for s in range(1, tp):
        squares = squares + ssq2[s]
    scale2 = lax.rsqrt(squares[:, :1] / (columns * tp) + epsilon)
    lines = []
    for p in range(2):
        take(drecv.at[p], dr_sem.at[p])
        acc = dsend[p, i].astype(F32)
        for s in range(1, kv):
            acc = acc + drecv[p, s - 1].astype(F32)
        part = scale2[p * eight : (p + 1) * eight]
        acc = (acc * (part * part)).astype(BF16).astype(F32)
        base = jnp.concatenate([own(p, a) for a in range(ratio)], axis=1)
        lines.append(base + acc)
    out_ref[...] = jnp.concatenate(lines, axis=0).astype(BF16)

    here = jnp.logical_and(owner == j, side == core)
    pl.when(here)(lambda: drain(xbuf.at[pl.ds(0, kv // 2 - 1)], hs_sem))
    pl.when(jnp.logical_not(here))(lambda: drain(xbuf.at[pl.ds(0, kv // 2)], hs_sem))
    drain(xbuf.at[pl.ds(0, kv // 2)], fs_sem)
    drain(ssq.at[pl.ds(0, tp - 1)], ss_sem)
    drain(prcv, ps_sem)
    drain(zrcv, qs_sem)
    drain(wrcv, ws_sem)
    drain(vrcv, es_sem)
    drain(mall.at[:, pl.ds(0, kv - 1)], ms_sem)
    drain(arecv, as_sem)
    pl.when(owner == j)(lambda: drain(rall.at[:, pl.ds(0, kv - 1)], rs_sem))
    pl.when(owner != j)(lambda: drain(rall, rs_sem))
    drain(ssq2.at[pl.ds(0, tp - 1)], ts_sem)
    drain(usend, us_sem)
    drain(xrecv, xs_sem)
    drain(act.at[:, 0], cs_sem)
    drain(drecv, ds_sem)


def layer(
    kv, tp, hidden_rows, carried, norm_gain, weights, decay_bias, head_gain, w_out, mlp_gain,
    w_up, w_down,
):
    rows, columns = hidden_rows.shape
    width = w_out.shape[1]
    ratio = kv // tp
    ny = inner_size(kv)
    nz = kv // ny
    cw = weights[0].shape[1]
    wide = weights[3].shape[1]
    pw = cw // SPLIT
    pieces = sum(w.shape[1] for w in weights) // pw
    late = LATE
    half = w_up.shape[1] // 2
    eight = rows // 2
    tokens = kv * eight
    chunks = max(1, min(CHUNKS, half // 128))
    piece = half // chunks
    limit = VMEM_BYTES - 4 * carried.size - 128 * 1024
    vmem = pl.BlockSpec(memory_space=pltpu.VMEM)
    hbm = pl.BlockSpec(memory_space=pltpu.HBM)
    dma = pltpu.SemaphoreType.DMA
    wq, wk, wd_, wv, wg = weights
    bias = decay_bias.reshape(1, -1)
    return pl.pallas_call(
        functools.partial(layer_kernel, kv, tp),
        out_shape=[
            pltpu.VMEM((rows, columns), BF16),
            pltpu.VMEM(carried.shape, F32),
        ],
        in_specs=[hbm] * 14,
        out_specs=[vmem, vmem],
        scratch_shapes=[
            pltpu.VMEM(a.shape, a.dtype)
            for a in (hidden_rows, norm_gain, bias, head_gain, mlp_gain)
        ]
        + [pltpu.VMEM((1, norm_gain.shape[0]), F32)]
        + [
            pltpu.VMEM(w.shape, BF16) for w in (wq, wk, wd_, wv, wg, w_out, w_up, w_down)
        ]
        + [
            pltpu.VMEM((kv, rows, width), BF16),
            pltpu.VMEM((pieces - late, ny, nz, rows, pw), BF16),
            pltpu.VMEM((pieces - late, ny - 1, nz, rows, pw), BF16),
            pltpu.VMEM((pieces - late, nz, rows, pw), BF16),
            pltpu.VMEM((pieces - late, nz - 1, rows, pw), BF16),
            pltpu.VMEM((late, nz, ny, rows, pw), BF16),
            pltpu.VMEM((late, nz - 1, ny, rows, pw), BF16),
            pltpu.VMEM((late, ny, rows, pw), BF16),
            pltpu.VMEM((late, ny - 1, rows, pw), BF16),
            pltpu.VMEM((tp, rows, 128), F32),
            pltpu.VMEM((rows, cw), F32),
            pltpu.VMEM((rows, cw), F32),
            pltpu.VMEM((rows, cw), F32),
            pltpu.VMEM((rows, wide), F32),
            pltpu.VMEM((rows, wide), F32),
            pltpu.VMEM((2, eight, wide), BF16),
            pltpu.VMEM((2, kv, eight, wide), BF16),
            pltpu.VMEM((2, tp, ratio * eight, width), BF16),
            pltpu.VMEM((2, tp - 1, ratio * eight, width), BF16),
            pltpu.VMEM((2, ratio * eight, width), BF16),
            pltpu.VMEM((2, kv, ratio * eight, width), BF16),
            pltpu.VMEM((2, chunks, tokens, piece), BF16),
            pltpu.VMEM((2, chunks, tokens, piece), BF16),
            pltpu.VMEM((2, chunks, tokens, piece), BF16),
            pltpu.VMEM((2, chunks, tp // 2 - 1, tokens, piece), BF16),
            pltpu.VMEM((2, 2, chunks, tokens, piece), BF16),
            pltpu.VMEM((2, kv, eight, columns), BF16),
            pltpu.VMEM((2, kv - 1, eight, columns), BF16),
            pltpu.VMEM((tp, rows, 128), F32),
            dma((5,)),
            dma((8,)),
            dma((kv // 2,)),
            dma((pieces - late,)),
            dma((pieces - late,)),
            dma((late,)),
            dma((late,)),
            dma((2,)),
            dma((2,)),
            dma((2,)),
            dma((2, chunks)),
            dma((2, chunks)),
            dma((2, chunks)),
            dma((2,)),
            dma((ONES,)),
        ],
        compiler_params=pltpu.CompilerParams(
            has_side_effects=True, collective_id=0, vmem_limit_bytes=limit
        ),
        name="layer",
    )(
        hidden_rows, norm_gain, bias, head_gain, mlp_gain, wq, wk, wd_, wv, wg, carried,
        w_out, w_up, w_down,
    )


def store_kernel(parts, new_in, rows_in, new_out, rows_out, sems):
    size = new_in.shape[1] // parts
    copies = [pltpu.make_async_copy(rows_in, rows_out, sems.at[parts])]
    for n in range(parts):
        at = pl.ds(n * size, size)
        copies.append(pltpu.make_async_copy(new_in.at[:, at], new_out.at[:, at], sems.at[n]))
    for copy in copies:
        copy.start()
    for copy in copies:
        copy.wait()


def store(updated_rows, new_state):
    parts = STORES
    vmem = pl.BlockSpec(memory_space=pltpu.VMEM)
    hbm = pl.BlockSpec(memory_space=pltpu.HBM)
    return pl.pallas_call(
        functools.partial(store_kernel, parts),
        out_shape=[
            jax.ShapeDtypeStruct(new_state.shape, new_state.dtype),
            jax.ShapeDtypeStruct(updated_rows.shape, updated_rows.dtype),
        ],
        in_specs=[vmem, vmem],
        out_specs=[hbm, hbm],
        scratch_shapes=[pltpu.SemaphoreType.DMA((parts + 1,))],
        compiler_params=pltpu.CompilerParams(vmem_limit_bytes=1024 * 1024),
        name="store",
    )(new_state, updated_rows)


def body(
    kv,
    tp,
    hidden_rows,
    carried_state,
    norm_gain,
    w_query,
    w_key,
    w_decay,
    w_value,
    w_gate,
    decay_bias,
    head_gain,
    w_out,
    mlp_gain,
    w_up,
    w_down,
):
    updated_rows, new_state = layer(
        kv, tp, hidden_rows, carried_state, norm_gain,
        (w_query, w_key, w_decay, w_value, w_gate), decay_bias, head_gain, w_out, mlp_gain,
        w_up, w_down,
    )
    new_state, updated_rows = store(updated_rows, new_state)
    return (updated_rows, new_state)


def solution(mesh):
    return jax.shard_map(
        functools.partial(body, mesh.shape["kv"], mesh.shape["tp"]),
        mesh=mesh,
        in_specs=(
            P("kv", "tp"),
            P("kv", "tp"),
            P(),
            P("kv", "tp"),
            P("kv", "tp"),
            P("kv", "tp"),
            P("kv", "tp"),
            P("kv", "tp"),
            P("tp"),
            P(),
            P("tp", "kv"),
            P("tp"),
            P("tp", "kv"),
            P("kv", "tp"),
        ),
        out_specs=(P("kv", "tp"), P("kv", "tp")),
        check_vma=False,
    )
```

```python
import functools

import jax
import jax.numpy as jnp
from jax import lax
from jax.experimental import pallas as pl
from jax.experimental.pallas import tpu as pltpu
from jax.sharding import PartitionSpec as P

DK = 128
DV = 256

epsilon = 1e-06
decay_normalizer = 16.0

F32 = jnp.float32
BF16 = jnp.bfloat16
MESH = pl.DeviceIdType.MESH
CHUNKS = 2
SPLIT = 1
LATE = 1
ONES = 19
STORES = 8
VMEM_BYTES = 67043328


def remote(src, dst, send_sem, recv_sem, i, j):
    return pltpu.make_async_remote_copy(
        src_ref=src,
        dst_ref=dst,
        send_sem=send_sem,
        recv_sem=recv_sem,
        device_id={"kv": i, "tp": j},
        device_id_type=MESH,
    )


def dot(a, b):
    return jnp.dot(a, b, preferred_element_type=F32)


def inner_size(kv):
    size = 1
    while (size * 2) ** 2 <= kv:
        size = size * 2
    return size


def layer_kernel(
    kv, tp,
    h_in, ng_in, bias_in, hg_in, mg_in, wq, wk, wd_, wv, wg, old, wo, wu, wdn,
    out_ref, st_ref,
    h_ref, ng_ref, bias_ref, hg_ref, mg_ref, gains,
    vq, vk, vd_, vv, vg, vo, vu, vdn,
    xbuf, psnd, prcv, zsnd, zrcv, wsnd, wrcv, vsnd, vrcv, ssq, query, key, decay, value, head,
    mixed, mall, asend, arecv, rpart, rall, usend, urecv, xsend, xrecv, act, dsend, drecv, ssq2,
    insem, wsem, hr_sem, pr_sem, qr_sem, wr_sem, er_sem, mr_sem, ar_sem, rr_sem,
    ur_sem, xr_sem, cr_sem, dr_sem, one,
):
    i, j = lax.axis_index("kv"), lax.axis_index("tp")
    ny = inner_size(kv)
    nz = kv // ny
    z, y = i // ny, lax.rem(i, ny)
    ratio = kv // tp
    owner = i // ratio
    rows = h_ref.shape[0]
    eight = rows // 2
    columns = h_ref.shape[1]
    width = xbuf.shape[2]
    cw = vq.shape[1]
    pw = psnd.shape[4]
    heads = cw // DK
    core = lax.rem(j, 2)
    across = j // 2
    other = 1 - core
    partner = across * 2 + other
    (
        st_sem, hs_sem, fs_sem, fr_sem, ss_sem, sr_sem, ps_sem, qs_sem, ws_sem, es_sem,
        ms_sem, as_sem, rs_sem, ts_sem, tr_sem, us_sem, xs_sem, cs_sem, ds_sem,
    ) = [one.at[n] for n in range(ONES)]

    def take(ref, sem):
        remote(ref, ref, sem, sem, i, partner).wait_recv()

    def drain(ref, sem):
        remote(ref, ref, sem, sem, i, partner).wait_send()

    def send(src, dst, send_sem, recv_sem, a, b):
        remote(src, dst, send_sem, recv_sem, a, b).start()

    upward = z < nz // 2
    far_z = [jnp.where(upward, n, nz - 1 - n) for n in range(nz)]

    def along_line(send_to):
        for zz in far_z:
            pl.when(zz != z)(functools.partial(send_to, zz, lax.rem(zz - z + nz, nz) - 1))

    def along_plane(send_to):
        for zz in far_z:
            for u in range(ny):
                k = zz * ny + lax.rem(y + u, ny)
                call = functools.partial(send_to, k, lax.rem(k - i + kv, kv) - 1)
                if u:
                    call()
                else:
                    pl.when(k != i)(call)

    inputs = [
        pltpu.make_async_copy(src, dst, insem.at[n])
        for n, (src, dst) in enumerate(
            ((h_in, h_ref), (ng_in, ng_ref), (bias_in, bias_ref), (hg_in, hg_ref), (mg_in, mg_ref))
        )
    ]
    for copy in inputs:
        copy.start()
    barrier = pltpu.get_barrier_semaphore()

    def greet(a, b):
        pl.semaphore_signal(
            barrier, inc=1, device_id={"kv": a, "tp": b}, device_id_type=MESH
        )

    for s in range(kv):
        k = lax.rem(i + s, kv)
        if s:
            greet(k, owner)
            greet(k, j)
        else:
            pl.when(owner != j)(lambda: greet(i, owner))
    for a in range(ratio):
        for s in range(tp):
            k, t = j * ratio + a, lax.rem(j + s, tp)
            if s:
                greet(k, t)
            else:
                pl.when(k != i)(functools.partial(greet, k, t))
    for s in range(1, tp):
        greet(i, lax.rem(j + s, tp))

    loads = [
        pltpu.make_async_copy(w, v, wsem.at[n])
        for n, (w, v) in enumerate(
            ((wd_, vd_), (wk, vk), (wq, vq), (wv, vv), (wg, vg), (wo, vo), (wu, vu), (wdn, vdn))
        )
    ]
    load_state = pltpu.make_async_copy(old, st_ref, st_sem)
    for load in loads[:5]:
        load.start()
    load_state.start()
    for load in loads[5:]:
        load.start()

    for copy in inputs:
        copy.wait()
    hidden = h_ref[...].astype(F32)
    ssq[j] = jnp.broadcast_to(jnp.sum(hidden * hidden, axis=1, keepdims=True), (rows, 128))
    itself = jnp.where(owner == j, 1, 0)
    pl.semaphore_wait(barrier, 2 * (kv - itself) + (kv - 1) + (tp - 1))

    side = lax.rem(i, 2)
    for a in range(ratio):
        k = j * ratio + a
        for s in range(tp // 2):
            t = lax.rem(across + s, tp // 2) * 2 + side
            copy = remote(
                h_ref.at[:, pl.ds(a * width, width)], xbuf.at[i], hs_sem, hr_sem.at[i // 2], k, t
            )
            if s:
                copy.start()
            else:
                here = jnp.logical_and(k == i, t == j)
                pl.when(jnp.logical_not(here))(copy.start)

                @pl.when(here)
                def _():
                    xbuf[i] = h_ref[:, a * width : (a + 1) * width]

    for s in range(1, tp):
        send(ssq.at[j], ssq.at[j], ss_sem, sr_sem, i, lax.rem(j + s, tp))

    gains[...] = ng_ref[...].astype(F32).reshape(1, kv * width)
    gain = gains[:, pl.ds(pl.multiple_of(i * width, 128), width)]
    for s in range(kv // 2):
        m = lax.rem(i // 2 + s, kv // 2)
        k = 2 * m + core
        if s:
            take(xbuf.at[k], hr_sem.at[m])
        else:
            pl.when(jnp.logical_or(owner != j, k != i))(lambda: take(xbuf.at[k], hr_sem.at[m]))
        send(xbuf.at[k], xbuf.at[k], fs_sem, fr_sem, i, partner)
    take(xbuf.at[pl.ds(0, kv // 2)], fr_sem)
    x = (xbuf[...].reshape(kv * rows, width).astype(F32) * gain).astype(BF16)

    pieces = []
    for n, v in enumerate((vd_, vk, vq, vv, vg)):
        for low in range(0, v.shape[1], pw):
            pieces.append((n, v, low))
    late = len(pieces) - wsnd.shape[0]
    ready = set()

    def product(c):
        n, v, low = pieces[c]
        if n not in ready:
            loads[n].wait()
            ready.add(n)
        return dot(x, v[:, low : low + pw]).astype(BF16)

    def first_z(c):
        part, e = product(c), c - late
        for zz in range(nz):
            for yy in range(ny):
                at = (zz * ny + yy) * rows
                wsnd[e, zz, yy] = part[at : at + rows]
        along_line(
            lambda zz, to: send(
                wsnd.at[e, zz], wrcv.at[e, to], ws_sem, wr_sem.at[e], zz * ny + y, j
            )
        )

    def first_y(c):
        part = product(c)
        for zz in range(nz):
            for yy in range(ny):
                at = (zz * ny + yy) * rows
                psnd[c, yy, zz] = part[at : at + rows]
        for s in range(1, ny):
            yy = lax.rem(y + s, ny)
            send(psnd.at[c, yy], prcv.at[c, s - 1], ps_sem, pr_sem.at[c], z * ny + yy, j)

    def then_y(c):
        e = c - late
        take(wrcv.at[e], wr_sem.at[e])
        acc = wsnd[e, z].astype(F32)
        for s in range(1, nz):
            acc = acc + wrcv[e, s - 1].astype(F32)
        vsnd[e] = acc.astype(BF16)
        for s in range(1, ny):
            yy = lax.rem(y + s, ny)
            send(vsnd.at[e, yy], vrcv.at[e, s - 1], es_sem, er_sem.at[e], z * ny + yy, j)

    def then_z(c):
        take(prcv.at[c], pr_sem.at[c])
        acc = psnd[c, y].astype(F32)
        for s in range(1, ny):
            acc = acc + prcv[c, s - 1].astype(F32)
        zsnd[c] = acc.astype(BF16)
        along_line(
            lambda zz, to: send(
                zsnd.at[c, zz], zrcv.at[c, to], qs_sem, qr_sem.at[c], zz * ny + y, j
            )
        )

    def reduced_piece(c):
        if c >= late:
            e = c - late
            take(vrcv.at[e], er_sem.at[e])
            acc = vsnd[e, y].astype(F32)
            for s in range(1, ny):
                acc = acc + vrcv[e, s - 1].astype(F32)
        else:
            take(zrcv.at[c], qr_sem.at[c])
            acc = zsnd[c, z].astype(F32)
            for s in range(1, nz):
                acc = acc + zrcv[c, s - 1].astype(F32)
        return (acc * scale).astype(BF16).astype(F32)

    def reduced(c):
        per = cw // pw
        return jnp.concatenate([reduced_piece(c * per + m) for m in range(per)], axis=1)

    def head_slices(h):
        narrow = pl.ds(pl.multiple_of(h * DK, DK), DK)
        wide = pl.ds(pl.multiple_of(h * DV, DV), DV)
        return narrow, wide

    def state_slice(h, c):
        return pl.ds(pl.multiple_of(h * (DK * DV) + c * DV, DV), DV)

    def read_state(low, high):
        @pl.loop(low, high)
        def _(h):
            narrow, wide = head_slices(h)
            q = query[:, narrow] * decay[:, narrow]
            acc = jnp.zeros((rows, DV), F32)
            for c in range(DK):
                acc = acc + q[:, c : c + 1] * st_ref[:, state_slice(h, c)]
            head[:, wide] = acc

    def write_state(low, high):
        @pl.loop(low, high)
        def _(h):
            narrow, wide = head_slices(h)
            k, d = key[:, narrow], decay[:, narrow]
            v = value[:, wide]
            for c in range(DK):
                at = state_slice(h, c)
                st_ref[:, at] = d[:, c : c + 1] * st_ref[:, at] + k[:, c : c + 1] * v

    first_y(0)
    for c in range(late, len(pieces)):
        first_z(c)
    for c in range(1, late):
        first_y(c)
    for c in range(late):
        if c == late - 1:
            for e in range(late, len(pieces)):
                then_y(e)
        then_z(c)
    take(ssq.at[pl.ds(0, tp - 1)], sr_sem)
    total = ssq[0]
    for s in range(1, tp):
        total = total + ssq[s]
    scale = lax.rsqrt(total[:, :1] / (kv * width) + epsilon)

    pre = reduced(0) + bias_ref[...]
    log_decay = jnp.minimum(pre, 0.0) - jnp.log1p(jnp.exp(-jnp.abs(pre)))
    decay[...] = jnp.exp(log_decay / decay_normalizer)
    key[...] = reduced(1)
    query[...] = reduced(2) * DK ** (-0.5)
    load_state.wait()
    read_state(0, heads)
    for c in range(3, 5):
        value[:, (c - 3) * cw : (c - 2) * cw] = reduced(c)
    head_gain = hg_ref[...].astype(F32).reshape(1, DV)
    for h in range(heads):
        at = slice(h * DK, (h + 1) * DK)
        weight = jnp.sum(query[:, at] * key[:, at], axis=1, keepdims=True)
        at = slice(h * DV, (h + 1) * DV)
        acc = head[:, at] + weight * value[:, at]
        acc = acc * lax.rsqrt(jnp.mean(acc * acc, axis=1, keepdims=True) + epsilon)
        head[:, at] = acc * head_gain

    for c in range(5, 7):
        at = slice((c - 5) * cw, (c - 4) * cw)
        both = head[:, at] * jax.nn.silu(reduced(c))
        for p in range(2):
            mixed[p, :, at] = both[p * eight : (p + 1) * eight].astype(BF16)

    for p in range(2):
        along_plane(
            lambda k, to: send(mixed.at[p], mall.at[p, i], ms_sem, mr_sem.at[p], k, j)
        )
    for p in range(2):
        mall[p, i] = mixed[p]
    write_state(0, heads // 2)

    loads[5].wait()
    tokens = kv * eight
    for p in range(2):
        take(mall.at[p, pl.ds(0, kv - 1)], mr_sem.at[p])
        every = mall[p].astype(F32).reshape(tokens, mall.shape[3]).astype(BF16)
        asend[p] = dot(every, vo[...]).astype(BF16).reshape(asend.shape[1:])
        for s in range(1, tp):
            t = lax.rem(j + s, tp)
            send(asend.at[p, t], arecv.at[p, s - 1], as_sem, ar_sem.at[p], i, t)
    slot = lax.rem(i, ratio)
    place = slot * tp + j
    mine = xbuf[pl.ds(j * ratio, ratio)].astype(F32)
    for p in range(2):
        take(arecv.at[p], ar_sem.at[p])
        attn = asend[p, j].astype(F32)
        for s in range(1, tp):
            attn = attn + arecv[p, s - 1].astype(F32)
        part = mine[:, p * eight : (p + 1) * eight].reshape(ratio * eight, width)
        rpart[p] = (part + attn.astype(BF16).astype(F32)).astype(BF16)
        give = lambda k, to: send(
            rpart.at[p], rall.at[p, place], rs_sem, rr_sem.at[p], k, owner
        )
        along_plane(give)
        pl.when(owner != j)(lambda: give(i, 0))

    @pl.when(owner == j)
    def _():
        for p in range(2):
            rall[p, place] = rpart[p]

    loads[6].wait()
    mlp_gain = mg_ref[...].astype(F32).reshape(1, columns)

    def gathered(p):
        pl.when(owner == j)(lambda: take(rall.at[p, pl.ds(0, kv - 1)], rr_sem.at[p]))
        pl.when(owner != j)(lambda: take(rall.at[p], rr_sem.at[p]))
        return jnp.concatenate(
            [
                (
                    rall[p, a * tp : (a + 1) * tp].reshape(tokens, width).astype(F32)
                    * mlp_gain[:, a * width : (a + 1) * width]
                ).astype(BF16)
                for a in range(ratio)
            ],
            axis=1,
        )

    def own(p, a):
        group = rall[p, a * tp + owner].astype(F32)
        value = group[:eight]
        for m in range(1, ratio):
            value = jnp.where(slot == m, group[m * eight : (m + 1) * eight], value)
        return value

    half = vu.shape[1] // 2
    chunks = usend.shape[1]
    piece = half // chunks

    def columns_of(h, c):
        return pl.ds(pl.multiple_of(h * half + c * piece, 128), piece)

    def up(p, x):
        def give(c):
            usend[p, c] = dot(x, vu[:, columns_of(other, c)]).astype(BF16)
            send(usend.at[p, c], urecv.at[p, c], us_sem, ur_sem.at[p, c], i, partner)

        give(0)
        for c in range(chunks):
            if c + 1 < chunks:
                give(c + 1)
            mine = dot(x, vu[:, columns_of(core, c)])
            take(urecv.at[p, c], ur_sem.at[p, c])
            xsend[p, c] = (mine + urecv[p, c].astype(F32)).astype(BF16)
            for s in range(1, tp // 2):
                to = lax.rem(across + s, tp // 2)
                send(
                    xsend.at[p, c], xrecv.at[p, c, s - 1], xs_sem, xr_sem.at[p, c],
                    i, to * 2 + core,
                )

    def down(p):
        acc = None
        for c in range(chunks):
            take(xrecv.at[p, c], xr_sem.at[p, c])
            total = xsend[p, c].astype(F32)
            for s in range(1, tp // 2):
                total = total + xrecv[p, c, s - 1].astype(F32)
            act[p, 0, c] = jnp.square(jnp.maximum(total, 0.0)).astype(BF16)
            send(act.at[p, 0, c], act.at[p, 1, c], cs_sem, cr_sem.at[p, c], i, partner)
            term = dot(act[p, 0, c], vdn[columns_of(core, c), :])
            acc = term if acc is None else acc + term
        for c in range(chunks):
            take(act.at[p, 1, c], cr_sem.at[p, c])
            acc = acc + dot(act[p, 1, c], vdn[columns_of(other, c), :])
        dsend[p] = acc.reshape(kv, eight, columns).astype(BF16)
        along_plane(
            lambda k, to: send(dsend.at[p, k], drecv.at[p, to], ds_sem, dr_sem.at[p], k, j)
        )

    x0 = gathered(0)
    up(0, x0)
    x1 = gathered(1)
    up(1, x1)
    squares = []
    for p in range(2):
        terms = [own(p, a) for a in range(ratio)]
        squares.append(sum(jnp.sum(term * term, axis=1, keepdims=True) for term in terms))
    squares = jnp.concatenate(squares, axis=0)
    ssq2[j] = jnp.broadcast_to(squares, (rows, 128))
    for s in range(1, tp):
        send(ssq2.at[j], ssq2.at[j], ts_sem, tr_sem, i, lax.rem(j + s, tp))
    loads[7].wait()
    down(0)
    down(1)
    write_state(heads // 2, heads)

    take(ssq2.at[pl.ds(0, tp - 1)], tr_sem)
    squares = ssq2[0]
    for s in range(1, tp):
        squares = squares + ssq2[s]
    scale2 = lax.rsqrt(squares[:, :1] / (columns * tp) + epsilon)
    lines = []
    for p in range(2):
        take(drecv.at[p], dr_sem.at[p])
        acc = dsend[p, i].astype(F32)
        for s in range(1, kv):
            acc = acc + drecv[p, s - 1].astype(F32)
        part = scale2[p * eight : (p + 1) * eight]
        acc = (acc * (part * part)).astype(BF16).astype(F32)
        base = jnp.concatenate([own(p, a) for a in range(ratio)], axis=1)
        lines.append(base + acc)
    out_ref[...] = jnp.concatenate(lines, axis=0).astype(BF16)

    here = jnp.logical_and(owner == j, side == core)
    pl.when(here)(lambda: drain(xbuf.at[pl.ds(0, kv // 2 - 1)], hs_sem))
    pl.when(jnp.logical_not(here))(lambda: drain(xbuf.at[pl.ds(0, kv // 2)], hs_sem))
    drain(xbuf.at[pl.ds(0, kv // 2)], fs_sem)
    drain(ssq.at[pl.ds(0, tp - 1)], ss_sem)
    drain(prcv, ps_sem)
    drain(zrcv, qs_sem)
    drain(wrcv, ws_sem)
    drain(vrcv, es_sem)
    drain(mall.at[:, pl.ds(0, kv - 1)], ms_sem)
    drain(arecv, as_sem)
    pl.when(owner == j)(lambda: drain(rall.at[:, pl.ds(0, kv - 1)], rs_sem))
    pl.when(owner != j)(lambda: drain(rall, rs_sem))
    drain(ssq2.at[pl.ds(0, tp - 1)], ts_sem)
    drain(usend, us_sem)
    drain(xrecv, xs_sem)
    drain(act.at[:, 0], cs_sem)
    drain(drecv, ds_sem)


def layer(
    kv, tp, hidden_rows, carried, norm_gain, weights, decay_bias, head_gain, w_out, mlp_gain,
    w_up, w_down,
):
    rows, columns = hidden_rows.shape
    width = w_out.shape[1]
    ratio = kv // tp
    ny = inner_size(kv)
    nz = kv // ny
    cw = weights[0].shape[1]
    wide = weights[3].shape[1]
    pw = cw // SPLIT
    pieces = sum(w.shape[1] for w in weights) // pw
    late = LATE
    half = w_up.shape[1] // 2
    eight = rows // 2
    tokens = kv * eight
    chunks = max(1, min(CHUNKS, half // 128))
    piece = half // chunks
    limit = VMEM_BYTES - 4 * carried.size - 128 * 1024
    vmem = pl.BlockSpec(memory_space=pltpu.VMEM)
    hbm = pl.BlockSpec(memory_space=pltpu.HBM)
    dma = pltpu.SemaphoreType.DMA
    wq, wk, wd_, wv, wg = weights
    bias = decay_bias.reshape(1, -1)
    return pl.pallas_call(
        functools.partial(layer_kernel, kv, tp),
        out_shape=[
            pltpu.VMEM((rows, columns), BF16),
            pltpu.VMEM(carried.shape, F32),
        ],
        in_specs=[hbm] * 14,
        out_specs=[vmem, vmem],
        scratch_shapes=[
            pltpu.VMEM(a.shape, a.dtype)
            for a in (hidden_rows, norm_gain, bias, head_gain, mlp_gain)
        ]
        + [pltpu.VMEM((1, norm_gain.shape[0]), F32)]
        + [
            pltpu.VMEM(w.shape, BF16) for w in (wq, wk, wd_, wv, wg, w_out, w_up, w_down)
        ]
        + [
            pltpu.VMEM((kv, rows, width), BF16),
            pltpu.VMEM((pieces - late, ny, nz, rows, pw), BF16),
            pltpu.VMEM((pieces - late, ny - 1, nz, rows, pw), BF16),
            pltpu.VMEM((pieces - late, nz, rows, pw), BF16),
            pltpu.VMEM((pieces - late, nz - 1, rows, pw), BF16),
            pltpu.VMEM((late, nz, ny, rows, pw), BF16),
            pltpu.VMEM((late, nz - 1, ny, rows, pw), BF16),
            pltpu.VMEM((late, ny, rows, pw), BF16),
            pltpu.VMEM((late, ny - 1, rows, pw), BF16),
            pltpu.VMEM((tp, rows, 128), F32),
            pltpu.VMEM((rows, cw), F32),
            pltpu.VMEM((rows, cw), F32),
            pltpu.VMEM((rows, cw), F32),
            pltpu.VMEM((rows, wide), F32),
            pltpu.VMEM((rows, wide), F32),
            pltpu.VMEM((2, eight, wide), BF16),
            pltpu.VMEM((2, kv, eight, wide), BF16),
            pltpu.VMEM((2, tp, ratio * eight, width), BF16),
            pltpu.VMEM((2, tp - 1, ratio * eight, width), BF16),
            pltpu.VMEM((2, ratio * eight, width), BF16),
            pltpu.VMEM((2, kv, ratio * eight, width), BF16),
            pltpu.VMEM((2, chunks, tokens, piece), BF16),
            pltpu.VMEM((2, chunks, tokens, piece), BF16),
            pltpu.VMEM((2, chunks, tokens, piece), BF16),
            pltpu.VMEM((2, chunks, tp // 2 - 1, tokens, piece), BF16),
            pltpu.VMEM((2, 2, chunks, tokens, piece), BF16),
            pltpu.VMEM((2, kv, eight, columns), BF16),
            pltpu.VMEM((2, kv - 1, eight, columns), BF16),
            pltpu.VMEM((tp, rows, 128), F32),
            dma((5,)),
            dma((8,)),
            dma((kv // 2,)),
            dma((pieces - late,)),
            dma((pieces - late,)),
            dma((late,)),
            dma((late,)),
            dma((2,)),
            dma((2,)),
            dma((2,)),
            dma((2, chunks)),
            dma((2, chunks)),
            dma((2, chunks)),
            dma((2,)),
            dma((ONES,)),
        ],
        compiler_params=pltpu.CompilerParams(
            has_side_effects=True, collective_id=0, vmem_limit_bytes=limit
        ),
        name="layer",
    )(
        hidden_rows, norm_gain, bias, head_gain, mlp_gain, wq, wk, wd_, wv, wg, carried,
        w_out, w_up, w_down,
    )


def store_kernel(parts, new_in, rows_in, new_out, rows_out, sems):
    size = new_in.shape[1] // parts
    copies = [pltpu.make_async_copy(rows_in, rows_out, sems.at[parts])]
    for n in range(parts):
        at = pl.ds(n * size, size)
        copies.append(pltpu.make_async_copy(new_in.at[:, at], new_out.at[:, at], sems.at[n]))
    for copy in copies:
        copy.start()
    for copy in copies:
        copy.wait()


def store(updated_rows, new_state):
    parts = STORES
    vmem = pl.BlockSpec(memory_space=pltpu.VMEM)
    hbm = pl.BlockSpec(memory_space=pltpu.HBM)
    return pl.pallas_call(
        functools.partial(store_kernel, parts),
        out_shape=[
            jax.ShapeDtypeStruct(new_state.shape, new_state.dtype),
            jax.ShapeDtypeStruct(updated_rows.shape, updated_rows.dtype),
        ],
        in_specs=[vmem, vmem],
        out_specs=[hbm, hbm],
        scratch_shapes=[pltpu.SemaphoreType.DMA((parts + 1,))],
        compiler_params=pltpu.CompilerParams(vmem_limit_bytes=1024 * 1024),
        name="store",
    )(new_state, updated_rows)


def body(
    kv,
    tp,
    hidden_rows,
    carried_state,
    norm_gain,
    w_query,
    w_key,
    w_decay,
    w_value,
    w_gate,
    decay_bias,
    head_gain,
    w_out,
    mlp_gain,
    w_up,
    w_down,
):
    updated_rows, new_state = layer(
        kv, tp, hidden_rows, carried_state, norm_gain,
        (w_query, w_key, w_decay, w_value, w_gate), decay_bias, head_gain, w_out, mlp_gain,
        w_up, w_down,
    )
    new_state, updated_rows = store(updated_rows, new_state)
    return (updated_rows, new_state)


def solution(mesh):
    return jax.shard_map(
        functools.partial(body, mesh.shape["kv"], mesh.shape["tp"]),
        mesh=mesh,
        in_specs=(
            P("kv", "tp"),
            P("kv", "tp"),
            P(),
            P("kv", "tp"),
            P("kv", "tp"),
            P("kv", "tp"),
            P("kv", "tp"),
            P("kv", "tp"),
            P("tp"),
            P(),
            P("tp", "kv"),
            P("tp"),
            P("tp", "kv"),
            P("kv", "tp"),
        ),
        out_specs=(P("kv", "tp"), P("kv", "tp")),
        check_vma=False,
    )
```
